32 devices in a mesh: fs: 8 (over z, x), tp: 4 (over y, core).
Axes of the slice: x: 2, y: 2, z: 4, core: 2. Of those that a mesh axis runs over, the one named last changes fastest.
Arguments:
- late_input: bfloat16 [4096, 2048], P(('fs', 'tp')), may hold values from -6 to 6
- norm_gain: bfloat16 [2048], replicated, may hold values from 0.099609375 to 1.8984375
- gate_weight: bfloat16 [2048, 2816], P('fs', 'tp'), may hold values from -0.125 to 0.125
- up_weight: bfloat16 [2048, 2816], P('fs', 'tp'), may hold values from -0.125 to 0.125
- down_weight: bfloat16 [2048, 2816], P('fs', 'tp'), may hold values from -0.109375 to 0.109375
- early_input: bfloat16 [4096, 2048], P(('fs', 'tp')), may hold values from -6 to 6
- cotangent: bfloat16 [4096, 2048], P(('fs', 'tp')), may hold values from -6 to 6
- gate_sum: float32 [2048, 2816], P('fs', 'tp'), may hold values from -192 to 192
- up_sum: float32 [2048, 2816], P('fs', 'tp'), may hold values from -192 to 192
- down_sum: float32 [2048, 2816], P('fs', 'tp'), may hold values from -192 to 192
- gain_sum: float32 [2048], replicated, may hold values from -192 to 192
Outputs:
- late_out: bfloat16 [4096, 2048], P(('fs', 'tp'))
- early_grad: bfloat16 [4096, 2048], P(('fs', 'tp'))
- gate_sum_out: float32 [2048, 2816], P('fs', 'tp')
- up_sum_out: float32 [2048, 2816], P('fs', 'tp')
- down_sum_out: float32 [2048, 2816], P('fs', 'tp')
- gain_sum_out: float32 [2048], replicated
The draws below stay inside these ranges and needn't reach their ends.
All inputs are finite; a program needn't handle non-finite values.
Results may differ from the reference program's by a relative error of at most 0.008.
Values may be sent and summed in bfloat16 or wider, within the bound.
A program may use at most 128 MiB of HBM per device.

```python
import jax
import jax.numpy as jnp
from jax import lax

D = 2048
FF = 2816
TOKENS = 4096
N_TP = 4


def with_spikes(drawn, stream_key, source, target, blocks, factor):
    owner, partner = [(jnp.arange(drawn.shape[axis_at]) // (drawn.shape[axis_at] // blocks)).reshape([-1 if axis == axis_at else 1 for axis in range(drawn.ndim)]) for axis_at in (source, target)]
    chosen = jax.random.permutation(stream_key, blocks)[partner]
    strong = (owner == chosen) | (owner == (partner + blocks // 2) % blocks)
    return jnp.where(strong, factor * drawn, drawn)


def block_levels(rng, extent, pieces, least, high):
    level = 1.0
    for axis_at, shards_of in pieces:
        draws = jax.random.uniform(jax.random.fold_in(jax.random.fold_in(rng, 6), axis_at), (shards_of,), jnp.float32, least / len(pieces), high / len(pieces))
        level = level * jnp.repeat(jnp.exp(draws), extent[axis_at] // shards_of).reshape((-1,) + (1,) * (len(extent) - 1 - axis_at))
    return level


def scatter_about(stream_key, shape, deviation, most, split=(), dtype=jnp.bfloat16):
    level = block_levels(stream_key, shape, split, -0.22, 0.18) if split else 1.0
    result = jax.random.normal(stream_key, shape, jnp.float32) * deviation * level
    return jnp.minimum(jnp.maximum(result, -most), most).astype(dtype)


def bell_draw_with(key, extent, deviation, limit, shards, heavy, dtype=jnp.bfloat16):
    entries = deviation * jax.random.normal(key, extent, jnp.float32)
    if shards:
        entries = entries * block_levels(key, extent, shards, -0.22, 0.18)
    return jnp.clip(with_spikes(entries, jax.random.fold_in(key, 3), *heavy), -limit, limit).astype(dtype)


def setup_inputs(seed: int = 0) -> dict:
    keys = jax.random.split(jax.random.key(seed), 12)
    return {
        "late_input": scatter_about(keys[0], (TOKENS, D), 1.0, 6.0, ((0, 32),)),
        "norm_gain": jnp.clip(1.0 + 0.18 * jax.random.normal(keys[1], (D,), jnp.float32), 0.099609375, 1.8984375).astype(jnp.bfloat16),
        "gate_weight": scatter_about(keys[2], (D, FF), D ** -0.5, 0.125, ((0, 8), (1, 4))),
        "up_weight": scatter_about(keys[3], (D, FF), D ** -0.5, 0.125, ((0, 8), (1, 4))),
        "down_weight": scatter_about(keys[4], (D, FF), FF ** -0.5, 0.109375, ((0, 8), (1, 4))),
        "early_input": scatter_about(keys[5], (TOKENS, D), 1.0, 6.0, ((0, 32),)),
        "cotangent": bell_draw_with(keys[6], (TOKENS, D), 1.0, 6.0, ((0, 32),), (0, 1, 32, 2.75)),
        "gate_sum": scatter_about(keys[7], (D, FF), 32.0, 192.0, ((0, 8), (1, 4)), jnp.float32),
        "up_sum": scatter_about(keys[8], (D, FF), 32.0, 192.0, ((0, 8), (1, 4)), jnp.float32),
        "down_sum": scatter_about(keys[9], (D, FF), 32.0, 192.0, ((0, 8), (1, 4)), jnp.float32),
        "gain_sum": scatter_about(keys[10], (D,), 32.0, 192.0, (), jnp.float32),
    }


epsilon = 1e-05

def normalize(source, gain_f):
    values = source.astype(jnp.float32)
    scale = lax.rsqrt(lax.optimization_barrier(jnp.mean(values * values, axis=-1, keepdims=True)) + epsilon)
    return ((values * scale * gain_f).astype(jnp.bfloat16), scale, values)

def blocked(pairs):
    width = FF // N_TP
    total = None
    for block in range(N_TP):
        partial_value = None
        for left, right in pairs:
            term = jnp.dot(left[:, block * width:(block + 1) * width], right[:, block * width:(block + 1) * width].T, preferred_element_type=jnp.float32)
            partial_value = term if partial_value is None else partial_value + term
        rounded = lax.optimization_barrier(partial_value.astype(jnp.bfloat16)).astype(jnp.float32)
        total = rounded if total is None else total + rounded
    return total

def reference(late_input, norm_gain, gate_weight, up_weight, down_weight, early_input, cotangent, gate_sum, up_sum, down_sum, gain_sum):
    gain_f = norm_gain.astype(jnp.float32)
    normed, scale, values = normalize(late_input, gain_f)
    gate = jnp.dot(normed, gate_weight, preferred_element_type=jnp.float32)
    upper = jnp.dot(normed, up_weight, preferred_element_type=jnp.float32)
    hidden = (jax.nn.silu(gate) * upper).astype(jnp.bfloat16)
    mixed = blocked([(hidden, down_weight)])
    late_out = (values + 0.5 * mixed).astype(jnp.bfloat16)
    normed_e, scale_e, values_e = normalize(early_input, gain_f)
    gate_e = jnp.dot(normed_e, gate_weight, preferred_element_type=jnp.float32)
    upper_e = jnp.dot(normed_e, up_weight, preferred_element_type=jnp.float32)
    sigma_e = jax.nn.sigmoid(gate_e)
    hidden_e = (gate_e * sigma_e * upper_e).astype(jnp.bfloat16)
    d_hidden = 0.5 * jnp.dot(cotangent, down_weight, preferred_element_type=jnp.float32)
    d_gate = (d_hidden * upper_e * sigma_e * (1.0 + gate_e * (1.0 - sigma_e))).astype(jnp.bfloat16)
    d_up = (d_hidden * gate_e * sigma_e).astype(jnp.bfloat16)
    d_normed = blocked([(d_gate, gate_weight), (d_up, up_weight)])
    scaled_grad = d_normed * gain_f
    early_grad = (cotangent.astype(jnp.float32) + scale_e * scaled_grad - values_e * scale_e ** 3 * lax.optimization_barrier(jnp.mean(values_e * scaled_grad, axis=-1, keepdims=True))).astype(jnp.bfloat16)
    gain_sum_out = gain_sum + lax.optimization_barrier(jnp.sum(d_normed * values_e * scale_e, axis=0))
    gate_sum_out = gate_sum + jnp.dot(normed_e.T, d_gate, preferred_element_type=jnp.float32)
    up_sum_out = up_sum + jnp.dot(normed_e.T, d_up, preferred_element_type=jnp.float32)
    down_sum_out = down_sum + 0.5 * jnp.dot(cotangent.T, hidden_e, preferred_element_type=jnp.float32)
    return (late_out, early_grad, gate_sum_out, up_sum_out, down_sum_out, gain_sum_out)
```

```python
import functools

import jax
import jax.numpy as jnp
from jax import lax
from jax.experimental import pallas as pl
from jax.experimental.pallas import tpu as pltpu
from jax.sharding import PartitionSpec as P

epsilon = 1e-05
MESH = pl.DeviceIdType.MESH
VMEM_LIMIT = 60 * 1024 * 1024
FUSED_LIMIT = 63 * 1024 * 1024


def ring_place(index, n):
    odd = lax.rem(index, 2)
    half = index // 2
    return (1 - odd) * half + odd * (n - 1 - half)


def ring_index(place, n):
    back = place // (n // 2)
    return (1 - back) * (2 * place) + back * (2 * (n - 1 - place) + 1)


def neighbours(n):
    place = ring_place(lax.axis_index("fs"), n)
    right = ring_index(lax.rem(place + 1, n), n)
    left = ring_index(lax.rem(place + n - 1, n), n)
    return place, right, left


def greet(n_tp, right, left):
    me_tp = lax.axis_index("tp")
    barrier = pltpu.get_barrier_semaphore()
    for target in (right, left):
        pl.semaphore_signal(barrier, inc=1, device_id=(target, me_tp), device_id_type=MESH)
    for away in range(1, n_tp):
        peer = lax.rem(me_tp + away, n_tp)
        pl.semaphore_signal(
            barrier, inc=1, device_id=(lax.axis_index("fs"), peer), device_id_type=MESH
        )
    pl.semaphore_wait(barrier, 2 + n_tp - 1)


def gather_kernel(n, n_tp, turned, *refs):
    gate_in, up_in, dn_in, late_in, early_in, cot_ref, gain_ref = refs[:7]
    gu_out, dn_out, late_all, early_out, cot_out, both_out, hid_out = refs[7:14]
    gate_buf, up_buf, gu_ref, dn_buf, dn_ref, late_buf, early_buf, late_ref = refs[14:22]
    gu_all, dn_all, early_all, cot_all, sum_gu, sum_dn = refs[22:28]
    send_sem, recv_sem, tp_send, tp_recv, own_sem, in_sem, out_sem = refs[28:]
    me_fs, me_tp = lax.axis_index("fs"), lax.axis_index("tp")
    tokens = late_in.shape[0]
    mine = pl.ds(pl.multiple_of(me_tp * tokens, tokens), tokens)
    rows, width = dn_ref.shape
    loads = [
        pltpu.make_async_copy(source, target, in_sem.at[k])
        for k, (source, target) in enumerate(
            (
                (gate_in, gate_buf),
                (up_in, up_buf),
                (early_in, early_buf),
                (late_in, late_buf),
                (dn_in, dn_buf),
                (cot_ref, cot_all.at[mine]),
            )
        )
    ]
    for copy in loads:
        copy.start()
    place, right, left = neighbours(n)
    greet(n_tp, right, left)
    half = rows // 2
    outs = (gu_out, dn_out)
    pairs = ((gu_ref, gu_all), (dn_ref, dn_all))

    def window(owner, way):
        return pl.ds(pl.multiple_of(owner * rows + way * half, half), half)

    def piece(step, c, way, first):
        block, whole = pairs[c]
        if way == 0:
            owner = ring_index(lax.rem(place - step + n, n), n)
            target = right
        else:
            owner = ring_index(lax.rem(place + step, n), n)
            target = left
        spot = whole.at[window(owner, way)]
        source = block.at[pl.ds(way * half, half)] if first else spot
        return pltpu.make_async_remote_copy(
            src_ref=source,
            dst_ref=spot,
            send_sem=send_sem.at[step, c, way],
            recv_sem=recv_sem.at[step, c, way],
            device_id=(target, me_tp),
            device_id_type=MESH,
        )

    token_pairs = (
        (early_all.at[mine], early_all),
        (cot_ref, cot_all),
        (late_ref, late_all),
    )

    def token_piece(a, away):
        block, whole = token_pairs[a]
        return pltpu.make_async_remote_copy(
            src_ref=block,
            dst_ref=whole.at[mine],
            send_sem=tp_send.at[a, away - 1],
            recv_sem=tp_recv.at[a, away - 1],
            device_id=(me_fs, lax.rem(me_tp + away, n_tp)),
            device_id_type=MESH,
        )

    def spread(a):
        for away in range(1, n_tp):
            token_piece(a, away).start()

    def arrived(a):
        for away in range(1, n_tp):
            token_piece(a, away).wait()

    def owner_of(step, way):
        if way == 0:
            return ring_index(lax.rem(place - step + n, n), n)
        return ring_index(lax.rem(place + step, n), n)

    def landed(step, c, way):
        some = window(owner_of(step + 1, way), way)
        return pltpu.make_async_copy(
            pairs[c][1].at[some], outs[c].at[some], out_sem.at[step, c, way]
        )

    totals = ((sum_gu, early_all), (sum_dn, cot_all))

    def add_rows(step, c):
        total, left = totals[c]
        for way in range(2):
            some = window(owner_of(step, way), way)
            total[...] += jnp.dot(
                left[:, some], pairs[c][1][some, :], preferred_element_type=jnp.float32
            )

    def norm(source, target, base):
        def part(k, carry):
            some = pl.ds(pl.multiple_of(k * 16, 16), 16)
            values = source[some, :].astype(jnp.float32)
            scale = lax.rsqrt(jnp.mean(values * values, axis=-1, keepdims=True) + epsilon)
            target[pl.ds(pl.multiple_of(base + k * 16, 16), 16), :] = (values * scale * gain_ref[...]).astype(jnp.bfloat16)
            return carry

        lax.fori_loop(0, tokens // 16, part, 0)

    def plain(buffer):
        return buffer[...].T if turned else buffer[...]

    loads[4].wait()
    dn_ref[...] = plain(dn_buf)
    for way in range(2):
        piece(0, 1, way, True).start()
    loads[0].wait()
    loads[1].wait()
    gu_ref[:, :width] = plain(gate_buf)
    gu_ref[:, width:] = plain(up_buf)
    for way in range(2):
        piece(0, 0, way, True).start()
    loads[2].wait()
    norm(early_buf, early_all, me_tp * tokens)
    spread(0)
    spread(1)
    loads[3].wait()
    norm(late_buf, late_ref, 0)
    spread(2)
    loads[5].wait()
    here = pl.ds(pl.multiple_of(me_fs * rows, rows), rows)
    gu_all[here, :] = gu_ref[...]
    dn_all[here, :] = dn_ref[...]
    sum_gu[...] = jnp.zeros_like(sum_gu)
    sum_dn[...] = jnp.zeros_like(sum_dn)
    own = [
        pltpu.make_async_copy(late_ref, late_all.at[mine], own_sem.at[0]),
        pltpu.make_async_copy(gu_ref, gu_out.at[here], own_sem.at[1]),
        pltpu.make_async_copy(dn_ref, dn_out.at[here], own_sem.at[2]),
    ]
    for copy in own:
        copy.start()
    keep = [
        pltpu.make_async_copy(early_all, early_out, own_sem.at[3]),
        pltpu.make_async_copy(cot_all, cot_out, own_sem.at[4]),
    ]

    def body(step, carry):
        for c in (1, 0):
            for way in range(2):
                piece(step - 1, c, way, False).wait_recv()
                piece(step, c, way, False).start()
                landed(step - 1, c, way).start()
            which = 1 - c

            @pl.when(step == n // 2)
            def _():
                arrived(which)
                keep[which].start()

            if turned:

                @pl.when(step >= n // 2)
                def _():
                    add_rows(2 * (step - n // 2), which)
                    add_rows(2 * (step - n // 2) + 1, which)

        return carry

    lax.fori_loop(1, n - 1, body, 0)
    if turned:
        for c in (1, 0):
            add_rows(n - 2, c)
    for c in (1, 0):
        for way in range(2):
            piece(n - 2, c, way, False).wait_recv()
            landed(n - 2, c, way).start()
            piece(0, c, way, True).wait_send()
        if turned:
            add_rows(n - 1, c)
        else:
            total, rest = totals[c]
            total[...] = jnp.dot(
                rest[...], pairs[c][1][...], preferred_element_type=jnp.float32
            )

    def finish(k, carry):
        some = pl.ds(pl.multiple_of(k * 64, 64), 64)
        gate, upper = sum_gu[some, :width], sum_gu[some, width:]
        sigma = 1.0 / (1.0 + jnp.exp(-gate))
        d_hidden = 0.5 * sum_dn[some, :]
        hid_out[some, :] = (gate * sigma * upper).astype(jnp.bfloat16)
        both_out[some, :width] = (
            d_hidden * upper * sigma * (1.0 + gate * (1.0 - sigma))
        ).astype(jnp.bfloat16)
        both_out[some, width:] = (d_hidden * gate * sigma).astype(jnp.bfloat16)
        return carry

    lax.fori_loop(0, n_tp * tokens // 64, finish, 0)

    def drain(step, carry):
        for c in (1, 0):
            for way in range(2):
                piece(step, c, way, False).wait_send()
        return carry

    lax.fori_loop(1, n - 1, drain, 0)

    def put(step, carry):
        for c in range(2):
            for way in range(2):
                landed(step, c, way).wait()
        return carry

    lax.fori_loop(0, n - 1, put, 0)
    for copy in own + keep:
        copy.wait()
    arrived(2)


def gather(n, n_tp, turned, gate, up, dn, late, early, cot, gain):
    rows, width = gate.shape[::-1] if turned else gate.shape
    tokens, depth = late.shape
    vmem = pl.BlockSpec(memory_space=pltpu.VMEM)
    hbm = pl.BlockSpec(memory_space=pl.ANY)
    bf16 = jnp.bfloat16
    return pl.pallas_call(
        functools.partial(gather_kernel, n, n_tp, turned),
        out_shape=[
            jax.ShapeDtypeStruct((n * rows, 2 * width), bf16),
            jax.ShapeDtypeStruct((n * rows, width), bf16),
        ]
        + [jax.ShapeDtypeStruct((n_tp * tokens, depth), bf16)] * 3
        + [
            jax.ShapeDtypeStruct((n_tp * tokens, 2 * width), bf16),
            jax.ShapeDtypeStruct((n_tp * tokens, width), bf16),
        ],
        in_specs=[hbm] * 6 + [vmem],
        out_specs=[hbm] * 5 + [vmem] * 2,
        scratch_shapes=[
            pltpu.VMEM(gate.shape, bf16),
            pltpu.VMEM(gate.shape, bf16),
            pltpu.VMEM((rows, 2 * width), bf16),
            pltpu.VMEM(gate.shape, bf16),
            pltpu.VMEM((rows, width), bf16),
        ]
        + [pltpu.VMEM((tokens, depth), bf16)] * 3
        + [
            pltpu.VMEM((n * rows, 2 * width), bf16),
            pltpu.VMEM((n * rows, width), bf16),
            pltpu.VMEM((n_tp * tokens, depth), bf16),
            pltpu.VMEM((n_tp * tokens, depth), bf16),
            pltpu.VMEM((n_tp * tokens, 2 * width), jnp.float32),
            pltpu.VMEM((n_tp * tokens, width), jnp.float32),
        ]
        + [
            pltpu.SemaphoreType.DMA((n - 1, 2, 2)),
            pltpu.SemaphoreType.DMA((n - 1, 2, 2)),
            pltpu.SemaphoreType.DMA((3, n_tp - 1)),
            pltpu.SemaphoreType.DMA((3, n_tp - 1)),
            pltpu.SemaphoreType.DMA((5,)),
            pltpu.SemaphoreType.DMA((6,)),
            pltpu.SemaphoreType.DMA((n - 1, 2, 2)),
        ],
        compiler_params=pltpu.CompilerParams(
            collective_id=0, has_side_effects=True, vmem_limit_bytes=VMEM_LIMIT
        ),
    )(gate, up, dn, late, early, cot, gain)


def reduce_kernel(n, n_tp, turned, *refs):
    early_side, cot_side, both_ref, hid_ref, gain_ref, early_all, gu_in, dn_in, late_in = refs[:9]
    gu_out, dn_out, mix_out, dnorm_out, gain_out = refs[9:14]
    gu_slots, dn_slots, gain_slots, gain_tp, gu_first, dn_first = refs[14:20]
    gu_all, dn_all, late_all, mix_ref, dnorm_ref, gain_sum = refs[20:26]
    send_sem, recv_sem, gain_send, gain_recv, tp_send, tp_recv, last_send, last_recv = refs[26:34]
    in_sem, own_sem = refs[34:]
    loads = [
        pltpu.make_async_copy(source, target, in_sem.at[k])
        for k, (source, target) in enumerate(
            ((gu_in, gu_all), (late_in, late_all), (dn_in, dn_all))
        )
    ]
    for copy in loads:
        copy.start()
    me_fs, me_tp = lax.axis_index("fs"), lax.axis_index("tp")
    place, right, left = neighbours(n)
    barrier = pltpu.get_barrier_semaphore()

    def greet_fs(away, carry):
        target = lax.rem(me_fs + away, n)
        pl.semaphore_signal(barrier, inc=1, device_id=(target, me_tp), device_id_type=MESH)
        return carry

    lax.fori_loop(1, n, greet_fs, 0)
    for away in range(1, n_tp):
        peer = lax.rem(me_tp + away, n_tp)
        pl.semaphore_signal(barrier, inc=1, device_id=(me_fs, peer), device_id_type=MESH)
    pl.semaphore_wait(barrier, n - 1 + n_tp - 1)
    width = dn_all.shape[1]
    half = gu_first.shape[1]
    rows = 2 * half
    tokens = late_all.shape[0] // n_tp
    sets = ((gu_first, gu_slots), (dn_first, dn_slots))
    factors = ((early_side, both_ref, 1.0), (cot_side, hid_ref, 0.5))

    def local(step, way):
        if way == 0:
            owner = ring_index(lax.rem(place - step - 1 + n, n), n)
        else:
            owner = ring_index(lax.rem(place + step + 1, n), n)
        return pl.ds(pl.multiple_of(owner * rows + way * half, half), half)

    def product(step, c, way):
        side, other, factor = factors[c]
        if turned:
            left, contract = side[:, local(step, way)], 0
        else:
            left, contract = side[local(step, way), :], 1
        return factor * lax.dot_general(
            left,
            other[...],
            (((contract,), (0,)), ((), ())),
            preferred_element_type=jnp.float32,
        )

    def piece(step, c, way, first, landed=False):
        start, slots = sets[c]
        source = start.at[way] if first else slots.at[way, step if landed else step - 1]
        return pltpu.make_async_remote_copy(
            src_ref=source,
            dst_ref=slots.at[way, step],
            send_sem=send_sem.at[step, c, way],
            recv_sem=recv_sem.at[step, c, way],
            device_id=((left if way else right), me_tp),
            device_id_type=MESH,
        )

    def gain_piece(away):
        return pltpu.make_async_remote_copy(
            src_ref=gain_slots.at[me_fs],
            dst_ref=gain_slots.at[me_fs],
            send_sem=gain_send.at[away - 1],
            recv_sem=gain_recv.at[away - 1],
            device_id=(lax.rem(me_fs + away, n), me_tp),
            device_id_type=MESH,
        )

    results = ((dnorm_ref, dnorm_out), (mix_ref, mix_out))

    def share(a, away):
        source, target = results[a]
        return pltpu.make_async_remote_copy(
            src_ref=source.at[away - 1],
            dst_ref=target.at[away - 1],
            send_sem=tp_send.at[a, away - 1],
            recv_sem=tp_recv.at[a, away - 1],
            device_id=(me_fs, lax.rem(me_tp + away, n_tp)),
            device_id_type=MESH,
        )

    def keep(a):
        source, target = results[a]
        return pltpu.make_async_copy(source.at[n_tp - 1], target.at[n_tp - 1], own_sem.at[a])

    def block_of(away):
        return pl.ds(pl.multiple_of(lax.rem(me_tp + away, n_tp) * tokens, tokens), tokens)

    def grad_block(away):
        some = block_of(away)
        part = lax.dot_general(
            both_ref[some, :],
            gu_all[...],
            (((1,), (1,)), ((), ())),
            preferred_element_type=jnp.float32,
        ).astype(jnp.bfloat16)
        dnorm_ref[away - 1] = part
        gain_sum[...] += jnp.sum(
            part.astype(jnp.float32) * early_all[some, :].astype(jnp.float32),
            axis=0,
            keepdims=True,
        )

    def late_block(away):
        both = jnp.dot(
            late_all[block_of(away), :], gu_all[...], preferred_element_type=jnp.float32
        )
        gate = both[:, :width]
        hidden = (gate / (1.0 + jnp.exp(-gate)) * both[:, width:]).astype(jnp.bfloat16)
        mix_ref[away - 1] = lax.dot_general(
            hidden, dn_all[...], (((1,), (1,)), ((), ())), preferred_element_type=jnp.float32
        ).astype(jnp.bfloat16)

    for c in range(2):
        for way in range(2):
            sets[c][0][way] = product(0, c, way).astype(jnp.bfloat16)
            piece(0, c, way, True).start()
    gain_sum[...] = jnp.zeros_like(gain_sum)
    for copy in loads:
        copy.wait()

    for c in range(2):
        (grad_block, late_block)[c](1)
        share(c, 1).start()

    def body(step, carry):
        for c in range(2):
            slots = sets[c][1]
            for way in range(2):
                term = product(step, c, way)
                piece(step - 1, c, way, False, True).wait_recv()
                slots[way, step - 1] = (
                    slots[way, step - 1].astype(jnp.float32) + term
                ).astype(jnp.bfloat16)
                piece(step, c, way, False).start()

            @pl.when(step < n_tp)
            def _():
                (grad_block, late_block)[c](step + 1)

            @pl.when(step < n_tp - 1)
            def _():
                share(c, step + 1).start()

            @pl.when(step == n_tp - 1)
            def _():
                keep(c).start()

        @pl.when(step == n_tp - 1)
        def _():
            gain_slots[me_fs] = gain_sum[...] / gain_ref[...]

            def send(away, inner):
                gain_piece(away).start()
                return inner

            lax.fori_loop(1, n, send, 0)

        return carry

    lax.fori_loop(1, n - 1, body, 0)

    def settle(away, inner):
        gain_piece(away).wait()
        return inner

    lax.fori_loop(1, n, settle, 0)
    gain_tp[me_tp] = lax.fori_loop(
        1, n, lambda k, total: total + gain_slots[k], gain_slots[0]
    )
    last = []
    for away in range(1, n_tp):
        peer = lax.rem(me_tp + away, n_tp)
        copy = pltpu.make_async_remote_copy(
            src_ref=gain_tp.at[me_tp],
            dst_ref=gain_tp.at[me_tp],
            send_sem=last_send.at[away - 1],
            recv_sem=last_recv.at[away - 1],
            device_id=(me_fs, peer),
            device_id_type=MESH,
        )
        copy.start()
        last.append(copy)
    for c in range(2):
        slots = sets[c][1]
        for way in range(2):
            term = product(n - 1, c, way)
            piece(n - 2, c, way, False, True).wait_recv()
            total = slots[way, n - 2].astype(jnp.float32) + term
            out = (gu_out, dn_out)[c]
            if turned:
                out[:, pl.ds(way * half, half)] = total.T
            else:
                out[pl.ds(way * half, half), :] = total
            piece(0, c, way, True).wait_send()
    for copy in last:
        copy.wait()
    total = gain_tp[0]
    for k in range(1, n_tp):
        total = total + gain_tp[k]
    gain_out[...] = total

    def drain(step, carry):
        for c in range(2):
            for way in range(2):
                piece(step, c, way, False).wait_send()
        return carry

    lax.fori_loop(1, n - 1, drain, 0)
    for a in range(2):
        keep(a).wait()
        for away in range(1, n_tp):
            share(a, away).wait()


def reduce(n, n_tp, turned, early_side, cot_side, both, hid, gain, early_all, gu_all, dn_all, late_all):
    rows = gu_all.shape[0] // n
    half = rows // 2
    width = dn_all.shape[1]
    shapes = [(rows, 2 * width), (rows, width)]
    if turned:
        shapes = [shape[::-1] for shape in shapes]
    depth = late_all.shape[1]
    tokens = late_all.shape[0] // n_tp
    vmem = pl.BlockSpec(memory_space=pltpu.VMEM)
    hbm = pl.BlockSpec(memory_space=pl.ANY)
    f32, bf16 = jnp.float32, jnp.bfloat16
    return pl.pallas_call(
        functools.partial(reduce_kernel, n, n_tp, turned),
        out_shape=[
            jax.ShapeDtypeStruct(shapes[0], f32),
            jax.ShapeDtypeStruct(shapes[1], f32),
            jax.ShapeDtypeStruct((n_tp, tokens, depth), bf16),
            jax.ShapeDtypeStruct((n_tp, tokens, depth), bf16),
            jax.ShapeDtypeStruct(gain.shape, f32),
        ],
        in_specs=[vmem] * 6 + [hbm] * 3,
        out_specs=[vmem, vmem, hbm, hbm, vmem],
        scratch_shapes=[
            pltpu.VMEM((2, n - 1, half, 2 * width), bf16),
            pltpu.VMEM((2, n - 1, half, width), bf16),
            pltpu.VMEM((n,) + gain.shape, f32),
            pltpu.VMEM((n_tp,) + gain.shape, f32),
            pltpu.VMEM((2, half, 2 * width), bf16),
            pltpu.VMEM((2, half, width), bf16),
            pltpu.VMEM(gu_all.shape, bf16),
            pltpu.VMEM(dn_all.shape, bf16),
            pltpu.VMEM(late_all.shape, bf16),
            pltpu.VMEM((n_tp, tokens, depth), bf16),
            pltpu.VMEM((n_tp, tokens, depth), bf16),
            pltpu.VMEM(gain.shape, f32),
            pltpu.SemaphoreType.DMA((n - 1, 2, 2)),
            pltpu.SemaphoreType.DMA((n - 1, 2, 2)),
            pltpu.SemaphoreType.DMA((n - 1,)),
            pltpu.SemaphoreType.DMA((n - 1,)),
            pltpu.SemaphoreType.DMA((2, n_tp - 1)),
            pltpu.SemaphoreType.DMA((2, n_tp - 1)),
            pltpu.SemaphoreType.DMA((n_tp - 1,)),
            pltpu.SemaphoreType.DMA((n_tp - 1,)),
            pltpu.SemaphoreType.DMA((3,)),
            pltpu.SemaphoreType.DMA((2,)),
        ],
        compiler_params=pltpu.CompilerParams(
            collective_id=1, has_side_effects=True, vmem_limit_bytes=VMEM_LIMIT
        ),
    )(early_side, cot_side, both, hid, gain, early_all, gu_all, dn_all, late_all)


def per_device_rings(
    n,
    n_tp,
    late_input,
    norm_gain,
    gate_weight,
    up_weight,
    down_weight,
    early_input,
    cotangent,
    gate_sum,
    up_sum,
    down_sum,
    gain_sum,
):
    gain_f = norm_gain.astype(jnp.float32)
    width = gate_weight.shape[1]
    depth = late_input.shape[1]
    turned = gate_weight.shape[0] % 256 == 0
    weights = [gate_weight, up_weight, down_weight]
    if turned:
        weights = [weight.T for weight in weights]
    gain_row = gain_f.reshape(1, depth)
    gu_all, down_all, late_all, early_all, cot_all, d_both, hidden_e = gather(
        n, n_tp, turned, *weights, late_input, early_input, cotangent, gain_row
    )
    sides = (early_all, cot_all) if turned else (early_all.T, cot_all.T)
    gu_grad, down_grad, mix_got, d_got, gain_total = reduce(
        n, n_tp, turned, *sides, d_both, hidden_e, gain_row, early_all, gu_all, down_all, late_all
    )
    if turned:
        gate_grad, up_grad, down_grad = gu_grad[:width].T, gu_grad[width:].T, down_grad.T
    else:
        gate_grad, up_grad = gu_grad[:, :width], gu_grad[:, width:]

    def gathered(got):
        total = got[0].astype(jnp.float32)
        for k in range(1, n_tp):
            total = total + got[k].astype(jnp.float32)
        return total

    values = late_input.astype(jnp.float32)
    values_e = early_input.astype(jnp.float32)
    scale_e = lax.rsqrt(jnp.mean(values_e * values_e, axis=-1, keepdims=True) + epsilon)
    late_out = (values + 0.5 * gathered(mix_got)).astype(jnp.bfloat16)
    scaled_grad = gathered(d_got) * gain_f
    early_grad = (
        cotangent.astype(jnp.float32)
        + scale_e * scaled_grad
        - values_e * scale_e**3 * jnp.mean(values_e * scaled_grad, axis=-1, keepdims=True)
    ).astype(jnp.bfloat16)
    return (
        late_out,
        early_grad,
        gate_sum + gate_grad,
        up_sum + up_grad,
        down_sum + down_grad,
        gain_sum + gain_total.reshape(depth),
    )


def fused_kernel(n, cuts, *refs):
    gate_in, up_in, dn_in, late_in, early_in, cot_in, gain_ref = refs[:7]
    sums_in, gain_sum_ref = refs[7:10], refs[10]
    late_out, early_out = refs[11:13]
    sum_outs, gain_out = refs[13:16], refs[16]
    wall, toks, early_raw, late_raw, sums, grad, pair, slots = refs[17:25]
    act_f, act_t, d_gate, d_up, hid_l, part = refs[25:31]
    from_x, from_y, diag_x, diag_y, gain_mine, gain_got, gain_z = refs[31:38]
    back_mine, back_got, back_send, back_recv = refs[38:42]
    load_sem, own_sem, swap_send, swap_recv, line_send, line_recv = refs[42:48]
    core_send, core_recv, tok_send, tok_recv, pair_send, pair_recv = refs[48:54]
    rs_send, rs_recv, xy_send, xy_recv, gain_send, gain_recv = refs[54:]
    nz = n // 2
    fs, tp = lax.axis_index("fs"), lax.axis_index("tp")
    z, x = fs // 2, lax.rem(fs, 2)
    y, c = tp // 2, lax.rem(tp, 2)
    weights = (gate_in, up_in, dn_in)
    tokens, depth = late_in.shape
    width, rows = gate_in.shape
    split = tokens // 2
    bf16, f32 = jnp.bfloat16, jnp.float32
    count = len(cuts)
    straight = x == c

    def at(z_at, x_at, y_at, c_at):
        return (2 * z_at + x_at, 2 * y_at + c_at)

    up_z, down_z = lax.rem(z + 1, nz), lax.rem(z + nz - 1, nz)
    partner = at(z, x, y, 1 - c)
    x_side = at(z, 1 - x, y, c)
    y_side = at(z, x, 1 - y, c)
    crossed = at(z, c, y, x)

    def send(source, target, send_sem, recv_sem, device):
        return pltpu.make_async_remote_copy(
            src_ref=source,
            dst_ref=target,
            send_sem=send_sem,
            recv_sem=recv_sem,
            device_id=device,
            device_id_type=MESH,
        )

    def hold(k):
        return pl.ds(cuts[k][0], cuts[k][1])

    def block(j, wide=1):
        return pl.ds(pl.multiple_of(j * rows, rows), wide * rows)

    def some(start, size):
        return pl.ds(pl.multiple_of(start, 16), size)

    def own_load(k, m):
        return pltpu.make_async_copy(
            weights[m].at[hold(k)], wall.at[m, hold(k), block(fs)], own_sem.at[k, m]
        )

    def swap(k, m):
        return send(
            weights[m].at[hold(k)],
            wall.at[m, hold(k), block(fs)],
            swap_send.at[k, m],
            swap_recv.at[k, m],
            crossed,
        )

    p_me, p_x, p_y = 2 * x + y, 2 * (1 - x) + y, 2 * x + 1 - y
    p_d = 3 - p_me

    def place(p, start=0, size=tokens):
        return some(p * tokens + start, size)

    loads = [
        pltpu.make_async_copy(source, target, load_sem.at[i])
        for i, (source, target) in enumerate(
            (
                (early_in, early_raw),
                (late_in, late_raw),
                (cot_in, toks.at[1, place(p_me)]),
                (sums_in[0], sums.at[0]),
                (sums_in[1], sums.at[1]),
                (sums_in[2], sums.at[2]),
            )
        )
    ]
    for copy in loads[:3]:
        copy.start()

    @pl.when(straight)
    def _():
        for k in range(count):
            for m in range(3):
                own_load(k, m).start()

    for copy in loads[3:]:
        copy.start()

    barrier = pltpu.get_barrier_semaphore()

    def greet_at(device):
        pl.semaphore_signal(barrier, inc=1, device_id=device, device_id_type=MESH)

    for away in range(1, nz):
        greet_at(at(lax.rem(z + away, nz), x, y, c))
    for device in (partner, x_side, y_side):
        greet_at(device)

    @pl.when(straight)
    def _():
        pl.semaphore_wait(barrier, nz - 1 + 3)

    @pl.when(x != c)
    def _():
        greet_at(crossed)
        pl.semaphore_wait(barrier, nz - 1 + 4)

    def tok(a, kind):
        if kind < 2:
            where = place(p_me)
        elif kind == 2:
            where = place(p_y, 0, split)
        else:
            where = place(p_x, split, tokens - split)
        spot = toks.at[a, where]
        source = cot_in if a == 1 and kind < 2 else spot
        return send(
            source, spot, tok_send.at[a, kind], tok_recv.at[a, kind], y_side if kind % 2 else x_side
        )

    def tok_forward(a):
        tok(a, 1).wait_recv()
        tok(a, 2).start()
        tok(a, 0).wait_recv()
        tok(a, 3).start()

    def tok_rest(a):
        tok(a, 2).wait_recv()
        tok(a, 3).wait_recv()

    def line(k, zs, way, dist):
        spot = wall.at[:, hold(k), block(2 * zs + c)]
        return send(
            spot,
            spot,
            line_send.at[k, way, dist - 1],
            line_recv.at[k, way, dist - 1],
            at(down_z if way else up_z, x, y, c),
        )

    def core_copy(k, zs):
        spot = wall.at[:, hold(k), block(2 * zs + c)]
        return send(spot, spot, core_send.at[k, zs], core_recv.at[k, zs], partner)

    def pump(k, d):
        if d == 0:

            @pl.when(straight)
            def _():
                for m in range(3):
                    own_load(k, m).wait()

            @pl.when(x != c)
            def _():
                for m in range(3):
                    swap(k, m).wait_recv()

            @pl.when(z < nz - 1)
            def _():
                line(k, z, 0, 1).start()

            @pl.when(z > 0)
            def _():
                line(k, z, 1, 1).start()

            core_copy(k, z).start()
            return

        @pl.when(z >= d)
        def _():
            line(k, z - d, 0, d).wait_recv()

            if d < nz - 1:

                @pl.when(z < nz - 1)
                def _():
                    line(k, z - d, 0, d + 1).start()

            core_copy(k, z - d).start()

        @pl.when(z + d < nz)
        def _():
            line(k, z + d, 1, d).wait_recv()

            if d < nz - 1:

                @pl.when(z > 0)
                def _():
                    line(k, z + d, 1, d + 1).start()

            core_copy(k, z + d).start()

    def weights_in(k):
        for zs in range(nz):
            core_copy(k, zs).wait_recv()

    def norm(source, a):
        def step(i, carry):
            values = source[some(i * 16, 16), :].astype(f32)
            scale = lax.rsqrt(jnp.mean(values * values, axis=-1, keepdims=True) + epsilon)
            toks[a, some(p_me * tokens + i * 16, 16), :] = (
                values * scale * gain_ref[...]
            ).astype(bf16)
            return carry

        lax.fori_loop(0, tokens // 16, step, 0)

    def dot(left, right, sides):
        return lax.dot_general(left, right, (sides, ((), ())), preferred_element_type=f32)

    def hidden_dots(k, pairs):
        size = cuts[k][1]
        for i, (a, m) in enumerate(pairs):
            act_f[i, :, :size] = dot(toks[a], wall[m, hold(k), :], ((1,), (1,)))

    def act_early(k):
        size = cuts[k][1]
        hidden_dots(k, ((0, 0), (0, 1), (1, 2)))

        def step(i, carry):
            part_of = pl.ds(pl.multiple_of(i * 128, 128), 128)
            gate, upper = act_f[0, part_of, :size], act_f[1, part_of, :size]
            sigma = 1.0 / (1.0 + jnp.exp(-gate))
            d_hidden = 0.5 * act_f[2, part_of, :size]
            hidden = (gate * sigma * upper).astype(bf16)
            dg = (d_hidden * upper * sigma * (1.0 + gate * (1.0 - sigma))).astype(bf16)
            du = (d_hidden * gate * sigma).astype(bf16)
            d_gate[part_of, hold(k)] = dg
            d_up[part_of, hold(k)] = du
            act_t[0, hold(k), part_of] = dg.T
            act_t[1, hold(k), part_of] = du.T
            act_t[2, hold(k), part_of] = hidden.T
            return carry

        lax.fori_loop(0, 4 * tokens // 128, step, 0)

    def act_late(k):
        size = cuts[k][1]
        hidden_dots(k, ((2, 0), (2, 1)))

        def step(i, carry):
            part_of = pl.ds(pl.multiple_of(i * 64, 64), 64)
            gate, upper = act_f[0, part_of, :size], act_f[1, part_of, :size]
            hid_l[part_of, hold(k)] = (gate / (1.0 + jnp.exp(-gate)) * upper).astype(bf16)
            return carry

        lax.fori_loop(0, 4 * tokens // 64, step, 0)

    def turn(i):
        near = (1 - lax.rem(i, 2)) * (nz - 1 - i // 2) + lax.rem(i, 2) * (i // 2)
        far = (z >= nz // 2).astype(jnp.int32)
        return (1 - far) * near + far * (nz - 1 - near)

    def pair_copy(k, zq):
        return send(
            grad.at[:, hold(k), block(2 * zq + 1 - c)],
            pair.at[:, hold(k), block(zq)],
            pair_send.at[k, zq],
            pair_recv.at[k, zq],
            partner,
        )

    def products(k):
        def step(i, carry):
            zq = turn(i)
            both = block(2 * zq, 2)
            for m in range(3):
                grad[m, hold(k), both] = dot(
                    act_t[m, hold(k), :], toks[m // 2, :, both], ((1,), (0,))
                ).astype(bf16)
            pair_copy(k, zq).start()
            return carry

        lax.fori_loop(0, nz, step, 0)

    def passing(k, zq, way):
        if way == 0:
            target, slot = up_z, zq
        else:
            last = (zq == z - 1).astype(jnp.int32)
            target, slot = down_z, last * nz + (1 - last) * zq
        return send(
            grad.at[:, hold(k), block(2 * zq + c)],
            slots.at[slot, :, hold(k), :],
            rs_send.at[k, zq],
            rs_recv.at[k, slot],
            at(target, x, y, c),
        )

    def landed(k, slot):
        here = slots.at[slot, :, hold(k), :]
        return send(here, here, rs_send.at[k, 0], rs_recv.at[k, slot], partner)

    def pass_on(k, zq):
        @pl.when(zq > z)
        def _():
            passing(k, zq, 0).start()

        @pl.when(zq < z)
        def _():
            passing(k, zq, 1).start()

    def upstream(zq):
        return ((zq > z) & (z > 0)) | ((zq < z) & (z < nz - 1))

    def combine_free(k):
        def step(i, carry):
            zq = turn(i)

            @pl.when((zq != z) & jnp.logical_not(upstream(zq)))
            def _():
                pair_copy(k, zq).wait_recv()
                for m in range(3):
                    spot = (m, hold(k), block(2 * zq + c))
                    grad[spot] = (
                        grad[spot].astype(f32) + pair[m, hold(k), block(zq)].astype(f32)
                    ).astype(bf16)
                pass_on(k, zq)

            return carry

        lax.fori_loop(0, nz, step, 0)

    def combine_up(k, i):
        zq = turn(jnp.int32(i))

        @pl.when((zq != z) & upstream(zq))
        def _():
            pair_copy(k, zq).wait_recv()
            landed(k, zq).wait_recv()
            for m in range(3):
                spot = (m, hold(k), block(2 * zq + c))
                grad[spot] = (
                    grad[spot].astype(f32)
                    + pair[m, hold(k), block(zq)].astype(f32)
                    + slots[zq, m, hold(k), :].astype(f32)
                ).astype(bf16)
            pass_on(k, zq)

    def back(k):
        spot = back_mine.at[:, hold(k), :]
        return send(
            spot, back_got.at[:, hold(k), :], back_send.at[k], back_recv.at[k], crossed
        )

    factors = (1.0, 1.0, 0.5)

    def finish(k):
        pair_copy(k, z).wait_recv()

        @pl.when(z > 0)
        def _():
            landed(k, z).wait_recv()

        @pl.when(z < nz - 1)
        def _():
            landed(k, nz).wait_recv()

        def total(m):
            return (
                grad[m, hold(k), block(2 * z + c)].astype(f32)
                + pair[m, hold(k), block(z)].astype(f32)
                + slots[z, m, hold(k), :].astype(f32)
                + slots[nz, m, hold(k), :].astype(f32)
            )

        @pl.when(straight)
        def _():
            for m in range(3):
                sum_outs[m][hold(k), :] = sums[m, hold(k), :] + factors[m] * total(m)

        @pl.when(x != c)
        def _():
            for m in range(3):
                back_mine[m, hold(k), :] = total(m).astype(bf16)
            back(k).start()

    def finish_back(k):
        @pl.when(x != c)
        def _():
            back(k).wait_recv()
            for m in range(3):
                sum_outs[m][hold(k), :] = sums[m, hold(k), :] + factors[m] * back_got[
                    m, hold(k), :
                ].astype(f32)

    low, high = (0, split), (split, tokens - split)

    def share(a, kind):
        def of(p, piece):
            return part.at[a, place(p, *piece)]

        source, target = (
            (of(p_d, low), diag_x.at[a]),
            (of(p_d, high), diag_y.at[a]),
            (of(p_x, low), from_x.at[a, pl.ds(*low)]),
            (of(p_y, high), from_y.at[a, pl.ds(*high)]),
            (of(p_x, high), from_x.at[a, pl.ds(*high)]),
            (of(p_y, low), from_y.at[a, pl.ds(*low)]),
        )[kind]
        device = (x_side, y_side, x_side, y_side, x_side, y_side)[kind]
        return send(source, target, xy_send.at[a, kind], xy_recv.at[a, kind], device)

    def half_of(side):
        return pl.ds(pl.multiple_of(side * 2 * tokens, 2 * tokens), 2 * tokens)

    def grad_half(side):
        where = half_of(side)
        both = (
            dot(d_gate[where, :], wall[0], ((1,), (0,)))
            + dot(d_up[where, :], wall[1], ((1,), (0,)))
        ).astype(bf16)
        part[0, where, :] = both

    def gain_half(side):
        def step(i, total):
            where = some(side * 2 * tokens + i * 16, 16)
            term = part[0, where, :].astype(f32) * toks[0, where, :].astype(f32)
            return total + term[:8] + term[8:]

        return lax.fori_loop(0, tokens // 8, step, jnp.zeros((8, depth), f32))

    def late_half(side):
        where = half_of(side)
        part[1, where, :] = dot(hid_l[where, :], wall[2], ((1,), (0,))).astype(bf16)

    def share_forward(a):
        share(a, 1).wait_recv()
        where = place(p_x, *high)
        part[a, where, :] = (part[a, where, :].astype(f32) + diag_y[a].astype(f32)).astype(bf16)
        share(a, 4).start()
        share(a, 0).wait_recv()
        where = place(p_y, *low)
        part[a, where, :] = (part[a, where, :].astype(f32) + diag_x[a].astype(f32)).astype(bf16)
        share(a, 5).start()

    def share_in(a):
        for kind in range(2, 6):
            share(a, kind).wait_recv()

    def own_total(a, i):
        where, mine = some(i * 16, 16), some(p_me * tokens + i * 16, 16)
        return (
            part[a, mine, :].astype(f32)
            + from_x[a, where, :].astype(f32)
            + from_y[a, where, :].astype(f32)
        )

    def write_late():
        def step(i, carry):
            where = some(i * 16, 16)
            late_out[where, :] = (
                late_raw[where, :].astype(f32) + 0.5 * own_total(1, i)
            ).astype(bf16)
            return carry

        lax.fori_loop(0, tokens // 16, step, 0)

    def write_early():
        def step(i, carry):
            where = some(i * 16, 16)
            values = early_raw[where, :].astype(f32)
            scale = lax.rsqrt(jnp.mean(values * values, axis=-1, keepdims=True) + epsilon)
            scaled = own_total(0, i) * gain_ref[...]
            mean = jnp.mean(values * scaled, axis=-1, keepdims=True)
            cot = toks[1, some(p_me * tokens + i * 16, 16), :].astype(f32)
            early_out[where, :] = (cot + scale * scaled - values * scale**3 * mean).astype(bf16)
            return carry

        lax.fori_loop(0, tokens // 16, step, 0)

    def gain_step(i):
        return send(
            gain_mine.at[i],
            gain_got.at[i],
            gain_send.at[i],
            gain_recv.at[i],
            (partner, x_side, y_side)[i],
        )

    def gain_away(away):
        return send(
            gain_z.at[z],
            gain_z.at[z],
            gain_send.at[2 + away],
            gain_recv.at[2 + away],
            at(lax.rem(z + away, nz), x, y, c),
        )

    def gain_next(i):
        gain_step(i).wait_recv()
        total = gain_mine[i] + gain_got[i]
        if i < 2:
            gain_mine[i + 1] = total
            gain_step(i + 1).start()
        else:
            gain_z[z] = total
            for away in range(1, nz):
                gain_away(away).start()

    @pl.when(x != c)
    def _():
        for m in range(3):
            swap(0, m).start()

    tok(1, 0).start()
    tok(1, 1).start()
    loads[0].wait()
    norm(early_raw, 0)
    tok(0, 0).start()
    tok(0, 1).start()
    pump(0, 0)
    loads[1].wait()
    norm(late_raw, 2)

    @pl.when(z == 0)
    def _():
        slots[0] = jnp.zeros_like(slots[0])

    @pl.when(z == nz - 1)
    def _():
        slots[nz] = jnp.zeros_like(slots[nz])

    tok_forward(1)
    pump(0, 1)
    tok_forward(0)

    @pl.when(x != c)
    def _():
        for k in range(1, count):
            for m in range(3):
                swap(k, m).start()

    tok(2, 0).start()
    tok(2, 1).start()
    for d in range(2, nz):
        pump(0, d)
    if count > 1:
        pump(1, 0)
    loads[2].wait()
    tok_rest(1)
    tok_rest(0)
    for k in range(count):
        weights_in(k)
        act_early(k)
        products(k)
        combine_free(k)
        if k == 0:
            tok_forward(2)
        if k < count - 1:
            for d in range(1, nz):
                pump(k + 1, d)
                combine_up(k, d - 1)
                if d == 1:
                    if k == 0:
                        tok_rest(2)
                    act_late(k)
            combine_up(k, nz - 1)
            if k + 2 < count:
                pump(k + 2, 0)
    if count == 1:
        tok_rest(2)
    act_late(count - 1)
    grad_half(1 - x)
    for kind in range(3):
        share(0, kind).start()
    late_half(1 - x)
    for kind in range(3):
        share(1, kind).start()
    grad_half(x)
    share(0, 3).start()
    late_half(x)
    share(1, 3).start()
    gain = jnp.sum(gain_half(1 - x) + gain_half(x), axis=0, keepdims=True)
    gain_mine[0] = gain / gain_ref[...]
    gain_step(0).start()
    for i in range(3):
        loads[3 + i].wait()
    for k in range(count - 1):
        finish(k)
    combine_up(count - 1, 0)
    share_forward(0)
    gain_next(0)
    combine_up(count - 1, 1)
    share_forward(1)
    gain_next(1)
    for i in range(2, nz):
        combine_up(count - 1, i)
    gain_next(2)
    share_in(0)
    write_early()
    share_in(1)
    write_late()
    for away in range(1, nz):
        gain_away(away).wait_recv()
    total = gain_z[0]
    for k in range(1, nz):
        total = total + gain_z[k]
    gain_out[...] = gain_sum_ref[...] + total
    finish(count - 1)
    for k in range(count):
        finish_back(k)

    for i in range(3):
        gain_step(i).wait_send()
    for away in range(1, nz):
        gain_away(away).wait_send()
    for a in range(3):
        for kind in range(4):
            tok(a, kind).wait_send()
    for a in range(2):
        for kind in range(6):
            share(a, kind).wait_send()
    for k in range(count):

        @pl.when(x != c)
        def _():
            for m in range(3):
                swap(k, m).wait_send()
            back(k).wait_send()

        for d in range(nz - 1):

            @pl.when((z >= d) & (z < nz - 1))
            def _():
                line(k, z - d, 0, d + 1).wait_send()

            @pl.when((z + d < nz) & (z > 0))
            def _():
                line(k, z + d, 1, d + 1).wait_send()

        for zs in range(nz):
            core_copy(k, zs).wait_send()
            pair_copy(k, zs).wait_send()

            @pl.when(zs != z)
            def _():
                passing(k, jnp.int32(zs), 0).wait_send()


def fused(n, cuts, gate, up, dn, late, early, cot, gain, sums, gain_sum):
    width, rows = gate.shape
    tokens, depth = late.shape
    nz, count = n // 2, len(cuts)
    most = max(size for _, size in cuts)
    vmem = pl.BlockSpec(memory_space=pltpu.VMEM)
    hbm = pl.BlockSpec(memory_space=pl.ANY)
    f32, bf16 = jnp.float32, jnp.bfloat16
    dma = pltpu.SemaphoreType.DMA
    crowd = 4 * tokens
    split = tokens // 2
    return pl.pallas_call(
        functools.partial(fused_kernel, n, cuts),
        out_shape=[jax.ShapeDtypeStruct((tokens, depth), bf16)] * 2
        + [jax.ShapeDtypeStruct((width, rows), f32)] * 3
        + [jax.ShapeDtypeStruct((1, depth), f32)],
        in_specs=[hbm] * 6 + [vmem] + [hbm] * 3 + [vmem],
        out_specs=[vmem] * 6,
        scratch_shapes=[
            pltpu.VMEM((3, width, depth), bf16),
            pltpu.VMEM((3, crowd, depth), bf16),
            pltpu.VMEM((tokens, depth), bf16),
            pltpu.VMEM((tokens, depth), bf16),
            pltpu.VMEM((3, width, rows), f32),
            pltpu.VMEM((3, width, depth), bf16),
            pltpu.VMEM((3, width, nz * rows), bf16),
            pltpu.VMEM((nz + 1, 3, width, rows), bf16),
            pltpu.VMEM((3, crowd, most), f32),
            pltpu.VMEM((3, width, crowd), bf16),
            pltpu.VMEM((crowd, width), bf16),
            pltpu.VMEM((crowd, width), bf16),
            pltpu.VMEM((crowd, width), bf16),
            pltpu.VMEM((2, crowd, depth), bf16),
            pltpu.VMEM((2, tokens, depth), bf16),
            pltpu.VMEM((2, tokens, depth), bf16),
            pltpu.VMEM((2, split, depth), bf16),
            pltpu.VMEM((2, tokens - split, depth), bf16),
            pltpu.VMEM((3, 1, depth), f32),
            pltpu.VMEM((3, 1, depth), f32),
            pltpu.VMEM((nz, 1, depth), f32),
            pltpu.VMEM((3, width, rows), bf16),
            pltpu.VMEM((3, width, rows), bf16),
            dma((count,)),
            dma((count,)),
            dma((6,)),
            dma((count, 3)),
            dma((count, 3)),
            dma((count, 3)),
            dma((count, 2, nz - 1)),
            dma((count, 2, nz - 1)),
            dma((count, nz)),
            dma((count, nz)),
            dma((3, 4)),
            dma((3, 4)),
            dma((count, nz)),
            dma((count, nz)),
            dma((count, nz)),
            dma((count, nz + 1)),
            dma((2, 6)),
            dma((2, 6)),
            dma((2 + nz,)),
            dma((2 + nz,)),
        ],
        compiler_params=pltpu.CompilerParams(
            collective_id=2, has_side_effects=True, vmem_limit_bytes=FUSED_LIMIT
        ),
    )(gate, up, dn, late, early, cot, gain, *sums, gain_sum)


def cut_hidden(width):
    first = min(width, -(-width // 256) * 128)
    return tuple(cut for cut in ((0, first), (first, width - first)) if cut[1])


def per_device_fused(n, args):
    late, norm_gain, gate, up, dn, early, cot, gate_sum, up_sum, dn_sum, gain_sum = args
    depth = late.shape[1]
    out = fused(
        n,
        cut_hidden(gate.shape[1]),
        gate.T,
        up.T,
        dn.T,
        late,
        early,
        cot,
        norm_gain.astype(jnp.float32).reshape(1, depth),
        (gate_sum.T, up_sum.T, dn_sum.T),
        gain_sum.reshape(1, depth),
    )
    late_out, early_grad, gate_out, up_out, dn_out, gain_out = out
    return late_out, early_grad, gate_out.T, up_out.T, dn_out.T, gain_out.reshape(depth)


def per_device(n, n_tp, *args):
    if n_tp == 4 and n % 2 == 0 and args[2].shape[0] % 128 == 0:
        return per_device_fused(n, args)
    return per_device_rings(n, n_tp, *args)


def solution(mesh):
    token = P(("fs", "tp"), None)
    weight = P("fs", "tp")
    return jax.shard_map(
        functools.partial(per_device, mesh.shape["fs"], mesh.shape["tp"]),
        mesh=mesh,
        in_specs=(token, P(), weight, weight, weight, token, token, weight, weight, weight, P()),
        out_specs=(token, token, weight, weight, weight, P()),
        check_vma=False,
    )
```

```python
import functools

import jax
import jax.numpy as jnp
from jax import lax
from jax.experimental import pallas as pl
from jax.experimental.pallas import tpu as pltpu
from jax.sharding import PartitionSpec as P

epsilon = 1e-05
MESH = pl.DeviceIdType.MESH
VMEM_LIMIT = 60 * 1024 * 1024
FUSED_LIMIT = 63 * 1024 * 1024


def ring_place(index, n):
    odd = lax.rem(index, 2)
    half = index // 2
    return (1 - odd) * half + odd * (n - 1 - half)


def ring_index(place, n):
    back = place // (n // 2)
    return (1 - back) * (2 * place) + back * (2 * (n - 1 - place) + 1)


def neighbours(n):
    place = ring_place(lax.axis_index("fs"), n)
    right = ring_index(lax.rem(place + 1, n), n)
    left = ring_index(lax.rem(place + n - 1, n), n)
    return place, right, left


def greet(n_tp, right, left):
    me_tp = lax.axis_index("tp")
    barrier = pltpu.get_barrier_semaphore()
    for target in (right, left):
        pl.semaphore_signal(barrier, inc=1, device_id=(target, me_tp), device_id_type=MESH)
    for away in range(1, n_tp):
        peer = lax.rem(me_tp + away, n_tp)
        pl.semaphore_signal(
            barrier, inc=1, device_id=(lax.axis_index("fs"), peer), device_id_type=MESH
        )
    pl.semaphore_wait(barrier, 2 + n_tp - 1)


def gather_kernel(n, n_tp, turned, *refs):
    gate_in, up_in, dn_in, late_in, early_in, cot_ref, gain_ref = refs[:7]
    gu_out, dn_out, late_all, early_out, cot_out, both_out, hid_out = refs[7:14]
    gate_buf, up_buf, gu_ref, dn_buf, dn_ref, late_buf, early_buf, late_ref = refs[14:22]
    gu_all, dn_all, early_all, cot_all, sum_gu, sum_dn = refs[22:28]
    send_sem, recv_sem, tp_send, tp_recv, own_sem, in_sem, out_sem = refs[28:]
    me_fs, me_tp = lax.axis_index("fs"), lax.axis_index("tp")
    tokens = late_in.shape[0]
    mine = pl.ds(pl.multiple_of(me_tp * tokens, tokens), tokens)
    rows, width = dn_ref.shape
    loads = [
        pltpu.make_async_copy(source, target, in_sem.at[k])
        for k, (source, target) in enumerate(
            (
                (gate_in, gate_buf),
                (up_in, up_buf),
                (early_in, early_buf),
                (late_in, late_buf),
                (dn_in, dn_buf),
                (cot_ref, cot_all.at[mine]),
            )
        )
    ]
    for copy in loads:
        copy.start()
    place, right, left = neighbours(n)
    greet(n_tp, right, left)
    half = rows // 2
    outs = (gu_out, dn_out)
    pairs = ((gu_ref, gu_all), (dn_ref, dn_all))

    def window(owner, way):
        return pl.ds(pl.multiple_of(owner * rows + way * half, half), half)

    def piece(step, c, way, first):
        block, whole = pairs[c]
        if way == 0:
            owner = ring_index(lax.rem(place - step + n, n), n)
            target = right
        else:
            owner = ring_index(lax.rem(place + step, n), n)
            target = left
        spot = whole.at[window(owner, way)]
        source = block.at[pl.ds(way * half, half)] if first else spot
        return pltpu.make_async_remote_copy(
            src_ref=source,
            dst_ref=spot,
            send_sem=send_sem.at[step, c, way],
            recv_sem=recv_sem.at[step, c, way],
            device_id=(target, me_tp),
            device_id_type=MESH,
        )

    token_pairs = (
        (early_all.at[mine], early_all),
        (cot_ref, cot_all),
        (late_ref, late_all),
    )

    def token_piece(a, away):
        block, whole = token_pairs[a]
        return pltpu.make_async_remote_copy(
            src_ref=block,
            dst_ref=whole.at[mine],
            send_sem=tp_send.at[a, away - 1],
            recv_sem=tp_recv.at[a, away - 1],
            device_id=(me_fs, lax.rem(me_tp + away, n_tp)),
            device_id_type=MESH,
        )

    def spread(a):
        for away in range(1, n_tp):
            token_piece(a, away).start()

    def arrived(a):
        for away in range(1, n_tp):
            token_piece(a, away).wait()

    def owner_of(step, way):
        if way == 0:
            return ring_index(lax.rem(place - step + n, n), n)
        return ring_index(lax.rem(place + step, n), n)

    def landed(step, c, way):
        some = window(owner_of(step + 1, way), way)
        return pltpu.make_async_copy(
            pairs[c][1].at[some], outs[c].at[some], out_sem.at[step, c, way]
        )

    totals = ((sum_gu, early_all), (sum_dn, cot_all))

    def add_rows(step, c):
        total, left = totals[c]
        for way in range(2):
            some = window(owner_of(step, way), way)
            total[...] += jnp.dot(
                left[:, some], pairs[c][1][some, :], preferred_element_type=jnp.float32
            )

    def norm(source, target, base):
        def part(k, carry):
            some = pl.ds(pl.multiple_of(k * 16, 16), 16)
            values = source[some, :].astype(jnp.float32)
            scale = lax.rsqrt(jnp.mean(values * values, axis=-1, keepdims=True) + epsilon)
            target[pl.ds(pl.multiple_of(base + k * 16, 16), 16), :] = (values * scale * gain_ref[...]).astype(jnp.bfloat16)
            return carry

        lax.fori_loop(0, tokens // 16, part, 0)

    def plain(buffer):
        return buffer[...].T if turned else buffer[...]

    loads[4].wait()
    dn_ref[...] = plain(dn_buf)
    for way in range(2):
        piece(0, 1, way, True).start()
    loads[0].wait()
    loads[1].wait()
    gu_ref[:, :width] = plain(gate_buf)
    gu_ref[:, width:] = plain(up_buf)
    for way in range(2):
        piece(0, 0, way, True).start()
    loads[2].wait()
    norm(early_buf, early_all, me_tp * tokens)
    spread(0)
    spread(1)
    loads[3].wait()
    norm(late_buf, late_ref, 0)
    spread(2)
    loads[5].wait()
    here = pl.ds(pl.multiple_of(me_fs * rows, rows), rows)
    gu_all[here, :] = gu_ref[...]
    dn_all[here, :] = dn_ref[...]
    sum_gu[...] = jnp.zeros_like(sum_gu)
    sum_dn[...] = jnp.zeros_like(sum_dn)
    own = [
        pltpu.make_async_copy(late_ref, late_all.at[mine], own_sem.at[0]),
        pltpu.make_async_copy(gu_ref, gu_out.at[here], own_sem.at[1]),
        pltpu.make_async_copy(dn_ref, dn_out.at[here], own_sem.at[2]),
    ]
    for copy in own:
        copy.start()
    keep = [
        pltpu.make_async_copy(early_all, early_out, own_sem.at[3]),
        pltpu.make_async_copy(cot_all, cot_out, own_sem.at[4]),
    ]

    def body(step, carry):
        for c in (1, 0):
            for way in range(2):
                piece(step - 1, c, way, False).wait_recv()
                piece(step, c, way, False).start()
                landed(step - 1, c, way).start()
            which = 1 - c

            @pl.when(step == n // 2)
            def _():
                arrived(which)
                keep[which].start()

            if turned:

                @pl.when(step >= n // 2)
                def _():
                    add_rows(2 * (step - n // 2), which)
                    add_rows(2 * (step - n // 2) + 1, which)

        return carry

    lax.fori_loop(1, n - 1, body, 0)
    if turned:
        for c in (1, 0):
            add_rows(n - 2, c)
    for c in (1, 0):
        for way in range(2):
            piece(n - 2, c, way, False).wait_recv()
            landed(n - 2, c, way).start()
            piece(0, c, way, True).wait_send()
        if turned:
            add_rows(n - 1, c)
        else:
            total, rest = totals[c]
            total[...] = jnp.dot(
                rest[...], pairs[c][1][...], preferred_element_type=jnp.float32
            )

    def finish(k, carry):
        some = pl.ds(pl.multiple_of(k * 64, 64), 64)
        gate, upper = sum_gu[some, :width], sum_gu[some, width:]
        sigma = 1.0 / (1.0 + jnp.exp(-gate))
        d_hidden = 0.5 * sum_dn[some, :]
        hid_out[some, :] = (gate * sigma * upper).astype(jnp.bfloat16)
        both_out[some, :width] = (
            d_hidden * upper * sigma * (1.0 + gate * (1.0 - sigma))
        ).astype(jnp.bfloat16)
        both_out[some, width:] = (d_hidden * gate * sigma).astype(jnp.bfloat16)
        return carry

    lax.fori_loop(0, n_tp * tokens // 64, finish, 0)

    def drain(step, carry):
        for c in (1, 0):
            for way in range(2):
                piece(step, c, way, False).wait_send()
        return carry

    lax.fori_loop(1, n - 1, drain, 0)

    def put(step, carry):
        for c in range(2):
            for way in range(2):
                landed(step, c, way).wait()
        return carry

    lax.fori_loop(0, n - 1, put, 0)
    for copy in own + keep:
        copy.wait()
    arrived(2)


def gather(n, n_tp, turned, gate, up, dn, late, early, cot, gain):
    rows, width = gate.shape[::-1] if turned else gate.shape
    tokens, depth = late.shape
    vmem = pl.BlockSpec(memory_space=pltpu.VMEM)
    hbm = pl.BlockSpec(memory_space=pl.ANY)
    bf16 = jnp.bfloat16
    return pl.pallas_call(
        functools.partial(gather_kernel, n, n_tp, turned),
        out_shape=[
            jax.ShapeDtypeStruct((n * rows, 2 * width), bf16),
            jax.ShapeDtypeStruct((n * rows, width), bf16),
        ]
        + [jax.ShapeDtypeStruct((n_tp * tokens, depth), bf16)] * 3
        + [
            jax.ShapeDtypeStruct((n_tp * tokens, 2 * width), bf16),
            jax.ShapeDtypeStruct((n_tp * tokens, width), bf16),
        ],
        in_specs=[hbm] * 6 + [vmem],
        out_specs=[hbm] * 5 + [vmem] * 2,
        scratch_shapes=[
            pltpu.VMEM(gate.shape, bf16),
            pltpu.VMEM(gate.shape, bf16),
            pltpu.VMEM((rows, 2 * width), bf16),
            pltpu.VMEM(gate.shape, bf16),
            pltpu.VMEM((rows, width), bf16),
        ]
        + [pltpu.VMEM((tokens, depth), bf16)] * 3
        + [
            pltpu.VMEM((n * rows, 2 * width), bf16),
            pltpu.VMEM((n * rows, width), bf16),
            pltpu.VMEM((n_tp * tokens, depth), bf16),
            pltpu.VMEM((n_tp * tokens, depth), bf16),
            pltpu.VMEM((n_tp * tokens, 2 * width), jnp.float32),
            pltpu.VMEM((n_tp * tokens, width), jnp.float32),
        ]
        + [
            pltpu.SemaphoreType.DMA((n - 1, 2, 2)),
            pltpu.SemaphoreType.DMA((n - 1, 2, 2)),
            pltpu.SemaphoreType.DMA((3, n_tp - 1)),
            pltpu.SemaphoreType.DMA((3, n_tp - 1)),
            pltpu.SemaphoreType.DMA((5,)),
            pltpu.SemaphoreType.DMA((6,)),
            pltpu.SemaphoreType.DMA((n - 1, 2, 2)),
        ],
        compiler_params=pltpu.CompilerParams(
            collective_id=0, has_side_effects=True, vmem_limit_bytes=VMEM_LIMIT
        ),
    )(gate, up, dn, late, early, cot, gain)


def reduce_kernel(n, n_tp, turned, *refs):
    early_side, cot_side, both_ref, hid_ref, gain_ref, early_all, gu_in, dn_in, late_in = refs[:9]
    gu_out, dn_out, mix_out, dnorm_out, gain_out = refs[9:14]
    gu_slots, dn_slots, gain_slots, gain_tp, gu_first, dn_first = refs[14:20]
    gu_all, dn_all, late_all, mix_ref, dnorm_ref, gain_sum = refs[20:26]
    send_sem, recv_sem, gain_send, gain_recv, tp_send, tp_recv, last_send, last_recv = refs[26:34]
    in_sem, own_sem = refs[34:]
    loads = [
        pltpu.make_async_copy(source, target, in_sem.at[k])
        for k, (source, target) in enumerate(
            ((gu_in, gu_all), (late_in, late_all), (dn_in, dn_all))
        )
    ]
    for copy in loads:
        copy.start()
    me_fs, me_tp = lax.axis_index("fs"), lax.axis_index("tp")
    place, right, left = neighbours(n)
    barrier = pltpu.get_barrier_semaphore()

    def greet_fs(away, carry):
        target = lax.rem(me_fs + away, n)
        pl.semaphore_signal(barrier, inc=1, device_id=(target, me_tp), device_id_type=MESH)
        return carry

    lax.fori_loop(1, n, greet_fs, 0)
    for away in range(1, n_tp):
        peer = lax.rem(me_tp + away, n_tp)
        pl.semaphore_signal(barrier, inc=1, device_id=(me_fs, peer), device_id_type=MESH)
    pl.semaphore_wait(barrier, n - 1 + n_tp - 1)
    width = dn_all.shape[1]
    half = gu_first.shape[1]
    rows = 2 * half
    tokens = late_all.shape[0] // n_tp
    sets = ((gu_first, gu_slots), (dn_first, dn_slots))
    factors = ((early_side, both_ref, 1.0), (cot_side, hid_ref, 0.5))

    def local(step, way):
        if way == 0:
            owner = ring_index(lax.rem(place - step - 1 + n, n), n)
        else:
            owner = ring_index(lax.rem(place + step + 1, n), n)
        return pl.ds(pl.multiple_of(owner * rows + way * half, half), half)

    def product(step, c, way):
        side, other, factor = factors[c]
        if turned:
            left, contract = side[:, local(step, way)], 0
        else:
            left, contract = side[local(step, way), :], 1
        return factor * lax.dot_general(
            left,
            other[...],
            (((contract,), (0,)), ((), ())),
            preferred_element_type=jnp.float32,
        )

    def piece(step, c, way, first, landed=False):
        start, slots = sets[c]
        source = start.at[way] if first else slots.at[way, step if landed else step - 1]
        return pltpu.make_async_remote_copy(
            src_ref=source,
            dst_ref=slots.at[way, step],
            send_sem=send_sem.at[step, c, way],
            recv_sem=recv_sem.at[step, c, way],
            device_id=((left if way else right), me_tp),
            device_id_type=MESH,
        )

    def gain_piece(away):
        return pltpu.make_async_remote_copy(
            src_ref=gain_slots.at[me_fs],
            dst_ref=gain_slots.at[me_fs],
            send_sem=gain_send.at[away - 1],
            recv_sem=gain_recv.at[away - 1],
            device_id=(lax.rem(me_fs + away, n), me_tp),
            device_id_type=MESH,
        )

    results = ((dnorm_ref, dnorm_out), (mix_ref, mix_out))

    def share(a, away):
        source, target = results[a]
        return pltpu.make_async_remote_copy(
            src_ref=source.at[away - 1],
            dst_ref=target.at[away - 1],
            send_sem=tp_send.at[a, away - 1],
            recv_sem=tp_recv.at[a, away - 1],
            device_id=(me_fs, lax.rem(me_tp + away, n_tp)),
            device_id_type=MESH,
        )

    def keep(a):
        source, target = results[a]
        return pltpu.make_async_copy(source.at[n_tp - 1], target.at[n_tp - 1], own_sem.at[a])

    def block_of(away):
        return pl.ds(pl.multiple_of(lax.rem(me_tp + away, n_tp) * tokens, tokens), tokens)

    def grad_block(away):
        some = block_of(away)
        part = lax.dot_general(
            both_ref[some, :],
            gu_all[...],
            (((1,), (1,)), ((), ())),
            preferred_element_type=jnp.float32,
        ).astype(jnp.bfloat16)
        dnorm_ref[away - 1] = part
        gain_sum[...] += jnp.sum(
            part.astype(jnp.float32) * early_all[some, :].astype(jnp.float32),
            axis=0,
            keepdims=True,
        )

    def late_block(away):
        both = jnp.dot(
            late_all[block_of(away), :], gu_all[...], preferred_element_type=jnp.float32
        )
        gate = both[:, :width]
        hidden = (gate / (1.0 + jnp.exp(-gate)) * both[:, width:]).astype(jnp.bfloat16)
        mix_ref[away - 1] = lax.dot_general(
            hidden, dn_all[...], (((1,), (1,)), ((), ())), preferred_element_type=jnp.float32
        ).astype(jnp.bfloat16)

    for c in range(2):
        for way in range(2):
            sets[c][0][way] = product(0, c, way).astype(jnp.bfloat16)
            piece(0, c, way, True).start()
    gain_sum[...] = jnp.zeros_like(gain_sum)
    for copy in loads:
        copy.wait()

    for c in range(2):
        (grad_block, late_block)[c](1)
        share(c, 1).start()

    def body(step, carry):
        for c in range(2):
            slots = sets[c][1]
            for way in range(2):
                term = product(step, c, way)
                piece(step - 1, c, way, False, True).wait_recv()
                slots[way, step - 1] = (
                    slots[way, step - 1].astype(jnp.float32) + term
                ).astype(jnp.bfloat16)
                piece(step, c, way, False).start()

            @pl.when(step < n_tp)
            def _():
                (grad_block, late_block)[c](step + 1)

            @pl.when(step < n_tp - 1)
            def _():
                share(c, step + 1).start()

            @pl.when(step == n_tp - 1)
            def _():
                keep(c).start()

        @pl.when(step == n_tp - 1)
        def _():
            gain_slots[me_fs] = gain_sum[...] / gain_ref[...]

            def send(away, inner):
                gain_piece(away).start()
                return inner

            lax.fori_loop(1, n, send, 0)

        return carry

    lax.fori_loop(1, n - 1, body, 0)

    def settle(away, inner):
        gain_piece(away).wait()
        return inner

    lax.fori_loop(1, n, settle, 0)
    gain_tp[me_tp] = lax.fori_loop(
        1, n, lambda k, total: total + gain_slots[k], gain_slots[0]
    )
    last = []
    for away in range(1, n_tp):
        peer = lax.rem(me_tp + away, n_tp)
        copy = pltpu.make_async_remote_copy(
            src_ref=gain_tp.at[me_tp],
            dst_ref=gain_tp.at[me_tp],
            send_sem=last_send.at[away - 1],
            recv_sem=last_recv.at[away - 1],
            device_id=(me_fs, peer),
            device_id_type=MESH,
        )
        copy.start()
        last.append(copy)
    for c in range(2):
        slots = sets[c][1]
        for way in range(2):
            term = product(n - 1, c, way)
            piece(n - 2, c, way, False, True).wait_recv()
            total = slots[way, n - 2].astype(jnp.float32) + term
            out = (gu_out, dn_out)[c]
            if turned:
                out[:, pl.ds(way * half, half)] = total.T
            else:
                out[pl.ds(way * half, half), :] = total
            piece(0, c, way, True).wait_send()
    for copy in last:
        copy.wait()
    total = gain_tp[0]
    for k in range(1, n_tp):
        total = total + gain_tp[k]
    gain_out[...] = total

    def drain(step, carry):
        for c in range(2):
            for way in range(2):
                piece(step, c, way, False).wait_send()
        return carry

    lax.fori_loop(1, n - 1, drain, 0)
    for a in range(2):
        keep(a).wait()
        for away in range(1, n_tp):
            share(a, away).wait()


def reduce(n, n_tp, turned, early_side, cot_side, both, hid, gain, early_all, gu_all, dn_all, late_all):
    rows = gu_all.shape[0] // n
    half = rows // 2
    width = dn_all.shape[1]
    shapes = [(rows, 2 * width), (rows, width)]
    if turned:
        shapes = [shape[::-1] for shape in shapes]
    depth = late_all.shape[1]
    tokens = late_all.shape[0] // n_tp
    vmem = pl.BlockSpec(memory_space=pltpu.VMEM)
    hbm = pl.BlockSpec(memory_space=pl.ANY)
    f32, bf16 = jnp.float32, jnp.bfloat16
    return pl.pallas_call(
        functools.partial(reduce_kernel, n, n_tp, turned),
        out_shape=[
            jax.ShapeDtypeStruct(shapes[0], f32),
            jax.ShapeDtypeStruct(shapes[1], f32),
            jax.ShapeDtypeStruct((n_tp, tokens, depth), bf16),
            jax.ShapeDtypeStruct((n_tp, tokens, depth), bf16),
            jax.ShapeDtypeStruct(gain.shape, f32),
        ],
        in_specs=[vmem] * 6 + [hbm] * 3,
        out_specs=[vmem, vmem, hbm, hbm, vmem],
        scratch_shapes=[
            pltpu.VMEM((2, n - 1, half, 2 * width), bf16),
            pltpu.VMEM((2, n - 1, half, width), bf16),
            pltpu.VMEM((n,) + gain.shape, f32),
            pltpu.VMEM((n_tp,) + gain.shape, f32),
            pltpu.VMEM((2, half, 2 * width), bf16),
            pltpu.VMEM((2, half, width), bf16),
            pltpu.VMEM(gu_all.shape, bf16),
            pltpu.VMEM(dn_all.shape, bf16),
            pltpu.VMEM(late_all.shape, bf16),
            pltpu.VMEM((n_tp, tokens, depth), bf16),
            pltpu.VMEM((n_tp, tokens, depth), bf16),
            pltpu.VMEM(gain.shape, f32),
            pltpu.SemaphoreType.DMA((n - 1, 2, 2)),
            pltpu.SemaphoreType.DMA((n - 1, 2, 2)),
            pltpu.SemaphoreType.DMA((n - 1,)),
            pltpu.SemaphoreType.DMA((n - 1,)),
            pltpu.SemaphoreType.DMA((2, n_tp - 1)),
            pltpu.SemaphoreType.DMA((2, n_tp - 1)),
            pltpu.SemaphoreType.DMA((n_tp - 1,)),
            pltpu.SemaphoreType.DMA((n_tp - 1,)),
            pltpu.SemaphoreType.DMA((3,)),
            pltpu.SemaphoreType.DMA((2,)),
        ],
        compiler_params=pltpu.CompilerParams(
            collective_id=1, has_side_effects=True, vmem_limit_bytes=VMEM_LIMIT
        ),
    )(early_side, cot_side, both, hid, gain, early_all, gu_all, dn_all, late_all)


def per_device_rings(
    n,
    n_tp,
    late_input,
    norm_gain,
    gate_weight,
    up_weight,
    down_weight,
    early_input,
    cotangent,
    gate_sum,
    up_sum,
    down_sum,
    gain_sum,
):
    gain_f = norm_gain.astype(jnp.float32)
    width = gate_weight.shape[1]
    depth = late_input.shape[1]
    turned = gate_weight.shape[0] % 256 == 0
    weights = [gate_weight, up_weight, down_weight]
    if turned:
        weights = [weight.T for weight in weights]
    gain_row = gain_f.reshape(1, depth)
    gu_all, down_all, late_all, early_all, cot_all, d_both, hidden_e = gather(
        n, n_tp, turned, *weights, late_input, early_input, cotangent, gain_row
    )
    sides = (early_all, cot_all) if turned else (early_all.T, cot_all.T)
    gu_grad, down_grad, mix_got, d_got, gain_total = reduce(
        n, n_tp, turned, *sides, d_both, hidden_e, gain_row, early_all, gu_all, down_all, late_all
    )
    if turned:
        gate_grad, up_grad, down_grad = gu_grad[:width].T, gu_grad[width:].T, down_grad.T
    else:
        gate_grad, up_grad = gu_grad[:, :width], gu_grad[:, width:]

    def gathered(got):
        total = got[0].astype(jnp.float32)
        for k in range(1, n_tp):
            total = total + got[k].astype(jnp.float32)
        return total

    values = late_input.astype(jnp.float32)
    values_e = early_input.astype(jnp.float32)
    scale_e = lax.rsqrt(jnp.mean(values_e * values_e, axis=-1, keepdims=True) + epsilon)
    late_out = (values + 0.5 * gathered(mix_got)).astype(jnp.bfloat16)
    scaled_grad = gathered(d_got) * gain_f
    early_grad = (
        cotangent.astype(jnp.float32)
        + scale_e * scaled_grad
        - values_e * scale_e**3 * jnp.mean(values_e * scaled_grad, axis=-1, keepdims=True)
    ).astype(jnp.bfloat16)
    return (
        late_out,
        early_grad,
        gate_sum + gate_grad,
        up_sum + up_grad,
        down_sum + down_grad,
        gain_sum + gain_total.reshape(depth),
    )


def fused_kernel(n, cuts, *refs):
    gate_in, up_in, dn_in, late_in, early_in, cot_in, gain_ref = refs[:7]
    sums_in, gain_sum_ref = refs[7:10], refs[10]
    token_outs, sum_outs, gain_out = refs[11:13], refs[13:16], refs[16]
    wall, toks, early_raw, late_raw, sums, grad, pair, slots = refs[17:25]
    act_f, act_t, d_gate, d_up, hid_l, part = refs[25:31]
    from_x, from_y, diag_x, diag_y, gain_mine, gain_got, gain_z = refs[31:38]
    back_mine, back_got, back_send, back_recv = refs[38:42]
    token_sem, sum_sem, gain_sem, gain_f = refs[-4:]
    load_sem, own_sem, swap_send, swap_recv, line_send, line_recv = refs[42:48]
    core_send, core_recv, tok_send, tok_recv, pair_send, pair_recv = refs[48:54]
    rs_send, rs_recv, xy_send, xy_recv, gain_send, gain_recv = refs[54:-4]
    nz = n // 2
    fs, tp = lax.axis_index("fs"), lax.axis_index("tp")
    z, x = fs // 2, lax.rem(fs, 2)
    y, c = tp // 2, lax.rem(tp, 2)
    weights = (gate_in, up_in, dn_in)
    tokens, depth = late_in.shape
    width, rows = gate_in.shape
    split = tokens * 3 // 128 * 16
    tok_splits = (16, split, tokens // 2)
    bf16, f32 = jnp.bfloat16, jnp.float32
    count = len(cuts)
    straight = x == c

    def at(z_at, x_at, y_at, c_at):
        return (2 * z_at + x_at, 2 * y_at + c_at)

    up_z, down_z = lax.rem(z + 1, nz), lax.rem(z + nz - 1, nz)
    partner = at(z, x, y, 1 - c)
    x_side = at(z, 1 - x, y, c)
    y_side = at(z, x, 1 - y, c)
    crossed = at(z, c, y, x)

    def send(source, target, send_sem, recv_sem, device):
        return pltpu.make_async_remote_copy(
            src_ref=source,
            dst_ref=target,
            send_sem=send_sem,
            recv_sem=recv_sem,
            device_id=device,
            device_id_type=MESH,
        )

    def hold(k):
        return pl.ds(cuts[k][0], cuts[k][1])

    def block(j, wide=1):
        return pl.ds(pl.multiple_of(j * rows, rows), wide * rows)

    def some(start, size):
        return pl.ds(pl.multiple_of(start, 16), size)

    def own_load(k, m):
        return pltpu.make_async_copy(
            weights[m].at[hold(k)], wall.at[m, hold(k), block(fs)], own_sem.at[k, m]
        )

    def swap(k, m):
        return send(
            weights[m].at[hold(k)],
            wall.at[m, hold(k), block(fs)],
            swap_send.at[k, m],
            swap_recv.at[k, m],
            crossed,
        )

    p_me, p_x, p_y = 2 * x + y, 2 * (1 - x) + y, 2 * x + 1 - y
    p_d = 3 - p_me

    def place(p, start=0, size=tokens):
        return some(p * tokens + start, size)

    loads = [
        pltpu.make_async_copy(source, target, load_sem.at[i])
        for i, (source, target) in enumerate(
            (
                (early_in, early_raw),
                (late_in, late_raw),
                (cot_in, toks.at[1, place(p_me)]),
                (sums_in[0], sums.at[0]),
                (sums_in[1], sums.at[1]),
                (sums_in[2], sums.at[2]),
            )
        )
    ]
    for copy in loads[:3]:
        copy.start()

    @pl.when(straight)
    def _():
        for k in range(count):
            for m in range(3):
                own_load(k, m).start()

    for copy in loads[3:]:
        copy.start()

    barrier = pltpu.get_barrier_semaphore()

    def greet_at(device):
        pl.semaphore_signal(barrier, inc=1, device_id=device, device_id_type=MESH)

    for away in range(1, nz):
        greet_at(at(lax.rem(z + away, nz), x, y, c))
    for device in (partner, x_side, y_side):
        greet_at(device)

    @pl.when(x != c)
    def _():
        greet_at(crossed)

    def tok(a, kind):
        cut = tok_splits[a]
        if kind < 2:
            where = place(p_me)
        elif kind == 2:
            where = place(p_y, 0, cut)
        else:
            where = place(p_x, cut, tokens - cut)
        spot = toks.at[a, where]
        source = cot_in if a == 1 and kind < 2 else spot
        return send(
            source, spot, tok_send.at[a, kind], tok_recv.at[a, kind], y_side if kind % 2 else x_side
        )

    def tok_over_x(a):
        tok(a, 1).wait_recv()
        tok(a, 2).start()

    def tok_over_y(a):
        tok(a, 0).wait_recv()
        tok(a, 3).start()

    def tok_rest(a):
        tok(a, 2).wait_recv()
        tok(a, 3).wait_recv()

    def line(k, zs, way, dist):
        spot = wall.at[:, hold(k), block(2 * zs + c)]
        return send(
            spot,
            spot,
            line_send.at[k, way, dist - 1],
            line_recv.at[k, way, dist - 1],
            at(down_z if way else up_z, x, y, c),
        )

    def core_copy(k, zs):
        spot = wall.at[:, hold(k), block(2 * zs + c)]
        return send(spot, spot, core_send.at[k, zs], core_recv.at[k, zs], partner)

    def pump(k, d):
        if d == 0:

            @pl.when(straight)
            def _():
                for m in range(3):
                    own_load(k, m).wait()

            @pl.when(x != c)
            def _():
                for m in range(3):
                    swap(k, m).wait_recv()

            core_copy(k, z).start()
            return

        @pl.when(z >= d)
        def _():
            line(k, z - d, 0, d).wait_recv()

            if d < nz - 1:

                @pl.when(z < nz - 1)
                def _():
                    line(k, z - d, 0, d + 1).start()

            core_copy(k, z - d).start()

        @pl.when(z + d < nz)
        def _():
            line(k, z + d, 1, d).wait_recv()

            if d < nz - 1:

                @pl.when(z > 0)
                def _():
                    line(k, z + d, 1, d + 1).start()

            core_copy(k, z + d).start()

    def lead(k):
        pump(k, 0)

        @pl.when(z == 0)
        def _():
            line(k, z, 0, 1).start()

        @pl.when(z == nz - 1)
        def _():
            line(k, z, 1, 1).start()

    def follow(k):
        @pl.when((z < nz - 1) & (z > 0))
        def _():
            line(k, z, 0, 1).start()
            line(k, z, 1, 1).start()

    def weights_in(k):
        for zs in range(nz):
            core_copy(k, zs).wait_recv()

    def norm(source, a):
        def step(i, carry):
            values = source[some(i * 16, 16), :].astype(f32)
            scale = lax.rsqrt(jnp.mean(values * values, axis=-1, keepdims=True) + epsilon)
            toks[a, some(p_me * tokens + i * 16, 16), :] = (
                values * scale * gain_f[...]
            ).astype(bf16)
            return carry

        lax.fori_loop(0, tokens // 16, step, 0)

    def dot(left, right, sides):
        return lax.dot_general(left, right, (sides, ((), ())), preferred_element_type=f32)

    def hidden_dots(k, triples):
        size = cuts[k][1]
        for i, a, m in triples:
            act_f[i, :, :size] = dot(toks[a], wall[m, hold(k), :], ((1,), (1,)))

    def act_first(k):
        hidden_dots(k, ((0, 0, 0), (1, 0, 1)))

    def act_second(k):
        size = cuts[k][1]
        hidden_dots(k, ((2, 1, 2),))

        def step(i, carry):
            part_of = pl.ds(pl.multiple_of(i * 128, 128), 128)
            gate, upper = act_f[0, part_of, :size], act_f[1, part_of, :size]
            sigma = 1.0 / (1.0 + jnp.exp(-gate))
            d_hidden = 0.5 * act_f[2, part_of, :size]
            hidden = (gate * sigma * upper).astype(bf16)
            dg = (d_hidden * upper * sigma * (1.0 + gate * (1.0 - sigma))).astype(bf16)
            du = (d_hidden * gate * sigma).astype(bf16)
            d_gate[part_of, hold(k)] = dg
            d_up[part_of, hold(k)] = du
            act_t[0, hold(k), part_of] = dg.T
            act_t[1, hold(k), part_of] = du.T
            act_t[2, hold(k), part_of] = hidden.T
            return carry

        lax.fori_loop(0, 4 * tokens // 128, step, 0)

    def act_late(k):
        size = cuts[k][1]
        hidden_dots(k, ((0, 2, 0), (1, 2, 1)))

        def step(i, carry):
            part_of = pl.ds(pl.multiple_of(i * 64, 64), 64)
            gate, upper = act_f[0, part_of, :size], act_f[1, part_of, :size]
            hid_l[part_of, hold(k)] = (gate / (1.0 + jnp.exp(-gate)) * upper).astype(bf16)
            return carry

        lax.fori_loop(0, 4 * tokens // 64, step, 0)

    def turn(i):
        near = (1 - lax.rem(i, 2)) * (nz - 1 - i // 2) + lax.rem(i, 2) * (i // 2)
        far = (z >= nz // 2).astype(jnp.int32)
        return (1 - far) * near + far * (nz - 1 - near)

    def pair_copy(k, zq):
        return send(
            grad.at[:, hold(k), block(2 * zq + 1 - c)],
            pair.at[:, hold(k), block(zq)],
            pair_send.at[k, zq],
            pair_recv.at[k, zq],
            partner,
        )

    def products(k):
        def step(i, carry):
            zq = turn(i)
            both = block(2 * zq, 2)
            gains = jnp.zeros((1, 2 * rows), f32)
            for m in range(3):
                term = dot(act_t[m, hold(k), :], toks[m // 2, :, both], ((1,), (0,)))
                grad[m, hold(k), both] = term.astype(bf16)
                if m < 2:
                    gains += jnp.sum(
                        term * wall[m, hold(k), both].astype(f32), axis=0, keepdims=True
                    )
            pair_copy(k, zq).start()
            gain_mine[0, :, both] += gains
            return carry

        lax.fori_loop(0, nz, step, 0)

    def passing(k, zq, way):
        if way == 0:
            target, slot = up_z, zq
        else:
            last = (zq == z - 1).astype(jnp.int32)
            target, slot = down_z, last * nz + (1 - last) * zq
        return send(
            grad.at[:, hold(k), block(2 * zq + c)],
            slots.at[slot, :, hold(k), :],
            rs_send.at[k, zq],
            rs_recv.at[k, slot],
            at(target, x, y, c),
        )

    def landed(k, slot):
        here = slots.at[slot, :, hold(k), :]
        return send(here, here, rs_send.at[k, 0], rs_recv.at[k, slot], partner)

    def pass_on(k, zq):
        @pl.when(zq > z)
        def _():
            passing(k, zq, 0).start()

        @pl.when(zq < z)
        def _():
            passing(k, zq, 1).start()

    def upstream(zq):
        return ((zq > z) & (z > 0)) | ((zq < z) & (z < nz - 1))

    def combine_free(k):
        def step(i, carry):
            zq = turn(i)

            @pl.when((zq != z) & jnp.logical_not(upstream(zq)))
            def _():
                pair_copy(k, zq).wait_recv()
                for m in range(3):
                    spot = (m, hold(k), block(2 * zq + c))
                    grad[spot] = (
                        grad[spot].astype(f32) + pair[m, hold(k), block(zq)].astype(f32)
                    ).astype(bf16)
                pass_on(k, zq)

            return carry

        lax.fori_loop(0, nz, step, 0)

    def combine_up(k, i):
        zq = turn(jnp.int32(i))

        @pl.when((zq != z) & upstream(zq))
        def _():
            pair_copy(k, zq).wait_recv()
            landed(k, zq).wait_recv()
            for m in range(3):
                spot = (m, hold(k), block(2 * zq + c))
                grad[spot] = (
                    grad[spot].astype(f32)
                    + pair[m, hold(k), block(zq)].astype(f32)
                    + slots[zq, m, hold(k), :].astype(f32)
                ).astype(bf16)
            pass_on(k, zq)

    def back(k):
        spot = back_mine.at[:, hold(k), :]
        return send(
            spot, back_got.at[:, hold(k), :], back_send.at[k], back_recv.at[k], crossed
        )

    factors = (1.0, 1.0, 0.5)

    def put(k, m):
        return pltpu.make_async_copy(
            sums.at[m, hold(k), :], sum_outs[m].at[hold(k), :], sum_sem.at[k, m]
        )

    def put_tokens(a):
        return pltpu.make_async_copy((early_raw, late_raw)[a], token_outs[1 - a], token_sem.at[a])

    def finish(k):
        pair_copy(k, z).wait_recv()

        @pl.when(z > 0)
        def _():
            landed(k, z).wait_recv()

        @pl.when(z < nz - 1)
        def _():
            landed(k, nz).wait_recv()

        def total(m):
            return (
                grad[m, hold(k), block(2 * z + c)].astype(f32)
                + pair[m, hold(k), block(z)].astype(f32)
                + slots[z, m, hold(k), :].astype(f32)
                + slots[nz, m, hold(k), :].astype(f32)
            )

        @pl.when(straight)
        def _():
            for m in range(3):
                sums[m, hold(k), :] += factors[m] * total(m)
                put(k, m).start()

        @pl.when(x != c)
        def _():
            for m in range(3):
                back_mine[m, hold(k), :] = total(m).astype(bf16)
            back(k).start()

    def finish_back(k):
        @pl.when(x != c)
        def _():
            back(k).wait_recv()
            for m in range(3):
                sums[m, hold(k), :] += factors[m] * back_got[m, hold(k), :].astype(f32)
                put(k, m).start()

    low, high = (0, split), (split, tokens - split)

    def share(a, kind):
        def of(p, piece):
            return part.at[a, place(p, *piece)]

        source, target = (
            (of(p_d, low), diag_x.at[a]),
            (of(p_d, high), diag_y.at[a]),
            (of(p_x, low), from_x.at[a, pl.ds(*low)]),
            (of(p_y, high), from_y.at[a, pl.ds(*high)]),
            (of(p_x, high), from_x.at[a, pl.ds(*high)]),
            (of(p_y, low), from_y.at[a, pl.ds(*low)]),
        )[kind]
        device = (x_side, y_side, x_side, y_side, x_side, y_side)[kind]
        return send(source, target, xy_send.at[a, kind], xy_recv.at[a, kind], device)

    def half_of(side):
        return pl.ds(pl.multiple_of(side * 2 * tokens, 2 * tokens), 2 * tokens)

    def grad_half(side):
        where = half_of(side)
        both = (
            dot(d_gate[where, :], wall[0], ((1,), (0,)))
            + dot(d_up[where, :], wall[1], ((1,), (0,)))
        ).astype(bf16)
        part[0, where, :] = both

    def late_half(side):
        where = half_of(side)
        part[1, where, :] = dot(hid_l[where, :], wall[2], ((1,), (0,))).astype(bf16)

    def share_forward(a):
        share(a, 1).wait_recv()
        where = place(p_x, *high)
        part[a, where, :] = (part[a, where, :].astype(f32) + diag_y[a].astype(f32)).astype(bf16)
        share(a, 4).start()
        share(a, 0).wait_recv()
        where = place(p_y, *low)
        part[a, where, :] = (part[a, where, :].astype(f32) + diag_x[a].astype(f32)).astype(bf16)
        share(a, 5).start()

    def share_in(a):
        for kind in range(2, 6):
            share(a, kind).wait_recv()

    def own_total(a, i):
        where, mine = some(i * 16, 16), some(p_me * tokens + i * 16, 16)
        return (
            part[a, mine, :].astype(f32)
            + from_x[a, where, :].astype(f32)
            + from_y[a, where, :].astype(f32)
        )

    def write_late():
        def step(i, carry):
            where = some(i * 16, 16)
            late_raw[where, :] = (
                late_raw[where, :].astype(f32) + 0.5 * own_total(1, i)
            ).astype(bf16)
            return carry

        lax.fori_loop(0, tokens // 16, step, 0)

    def write_early():
        def step(i, carry):
            where = some(i * 16, 16)
            values = early_raw[where, :].astype(f32)
            scale = lax.rsqrt(jnp.mean(values * values, axis=-1, keepdims=True) + epsilon)
            scaled = own_total(0, i) * gain_f[...]
            mean = jnp.mean(values * scaled, axis=-1, keepdims=True)
            cot = toks[1, some(p_me * tokens + i * 16, 16), :].astype(f32)
            early_raw[where, :] = (cot + scale * scaled - values * scale**3 * mean).astype(bf16)
            return carry

        lax.fori_loop(0, tokens // 16, step, 0)

    def gain_step(i):
        return send(
            gain_mine.at[i],
            gain_got.at[i],
            gain_send.at[i],
            gain_recv.at[i],
            (partner, x_side, y_side)[i],
        )

    def gain_away(away):
        return send(
            gain_z.at[z],
            gain_z.at[z],
            gain_send.at[2 + away],
            gain_recv.at[2 + away],
            at(lax.rem(z + away, nz), x, y, c),
        )

    def gain_next(i):
        gain_step(i).wait_recv()
        total = gain_mine[i] + gain_got[i]
        if i < 2:
            gain_mine[i + 1] = total
            gain_step(i + 1).start()
        else:
            gain_z[z] = total
            for away in range(1, nz):
                gain_away(away).start()

    def each_step(steps):
        for step in steps:
            if step[1] == 0:
                lead(step[0])
                follow(step[0])
            elif step[1] < 0:
                (lead, follow)[step[1] + 2](step[0])
            else:
                pump(*step)

    def when_straight(*steps):
        @pl.when(straight)
        def _():
            each_step(steps)

    def when_crossed(*steps):
        @pl.when(x != c)
        def _():
            each_step(steps)

    inner = (z > 0) & (z < nz - 1)

    def when_inner(*steps):
        @pl.when(inner)
        def _():
            each_step(steps)

    def when_outer(*steps):
        @pl.when(jnp.logical_not(inner))
        def _():
            each_step(steps)

    gain_f[...] = gain_ref[...].astype(f32).reshape(1, depth)
    loads[0].wait()
    norm(early_raw, 0)

    @pl.when(straight)
    def _():
        pl.semaphore_wait(barrier, nz - 1 + 3)

    @pl.when(x != c)
    def _():
        pl.semaphore_wait(barrier, nz - 1 + 4)

    @pl.when(x != c)
    def _():
        for k in range(count):
            for m in range(3):
                swap(k, m).start()

    for a in range(2):
        tok(a, 1).start()

    @pl.when(x != c)
    def _():
        for a in range(2):
            tok(a, 0).start()

    when_straight((0, 0), (1, -2))
    loads[1].wait()
    norm(late_raw, 2)
    gain_mine[0] = jnp.zeros((1, depth), f32)

    @pl.when(z == 0)
    def _():
        slots[0] = jnp.zeros_like(slots[0])

    @pl.when(z == nz - 1)
    def _():
        slots[nz] = jnp.zeros_like(slots[nz])

    when_crossed((0, 0))
    when_straight((0, 1))

    @pl.when(straight)
    def _():
        for a in range(2):
            tok(a, 0).start()

    tok_over_x(0)
    when_straight((2, -2), (0, 2), (1, -1))
    when_crossed((1, -2), (0, 1))
    tok_over_y(0)
    when_straight((0, 3), (1, 1))
    when_crossed((2, -2), (0, 2), (1, -1))
    loads[2].wait()
    tok_over_x(1)
    tok_over_y(1)
    tok_rest(0)
    when_crossed((0, 3))
    weights_in(0)
    act_first(0)
    when_straight((1, 2), (2, -1))
    tok_rest(1)
    tok(2, 1).start()
    tok(2, 0).start()
    act_second(0)
    products(0)
    combine_free(0)
    when_crossed((1, 1), (1, 2), (2, -1))
    when_inner((2, 1))
    when_outer((1, 3))
    tok_over_x(2)
    tok_over_y(2)
    combine_up(0, 0)
    when_inner((2, 2))
    weights_in(1)
    act_first(1)
    act_second(1)
    products(1)
    combine_free(1)
    combine_up(0, 1)
    when_outer((2, 1), (2, 2), (2, 3))
    tok_rest(2)
    act_late(0)
    combine_up(0, 2)
    combine_up(0, 3)
    act_late(1)
    weights_in(2)
    act_first(2)
    act_second(2)
    products(2)
    gain_mine[0] = gain_mine[0] / gain_f[...]
    gain_step(0).start()
    grad_half(1 - x)
    gain_next(0)
    for kind in range(3):
        share(0, kind).start()
    act_late(2)
    gain_next(1)
    late_half(1 - x)
    for kind in range(3):
        share(1, kind).start()
    combine_free(2)
    combine_up(1, 0)
    grad_half(x)
    share(0, 3).start()
    late_half(x)
    share(1, 3).start()
    gain_next(2)
    combine_up(1, 1)
    share_forward(0)
    combine_up(1, 2)
    combine_up(1, 3)
    for i in range(3):
        loads[3 + i].wait()
    finish(0)
    combine_up(2, 0)
    share_forward(1)
    combine_up(2, 1)
    finish(1)
    combine_up(2, 2)
    combine_up(2, 3)
    finish(2)
    finish_back(0)
    share_in(0)
    write_early()
    put_tokens(0).start()
    share_in(1)
    write_late()
    put_tokens(1).start()
    for away in range(1, nz):
        gain_away(away).wait_recv()
    total = gain_z[0]
    for k in range(1, nz):
        total = total + gain_z[k]
    gain_got[2] = gain_sum_ref[...] + total
    put_gain = pltpu.make_async_copy(gain_got.at[2], gain_out, gain_sem)
    put_gain.start()
    finish_back(1)
    finish_back(2)

    put_gain.wait()
    for a in range(2):
        put_tokens(a).wait()
    for k in range(count):
        for m in range(3):
            put(k, m).wait()
    for i in range(3):
        gain_step(i).wait_send()
    for away in range(1, nz):
        gain_away(away).wait_send()
    for a in range(3):
        for kind in range(4):
            tok(a, kind).wait_send()
    for a in range(2):
        for kind in range(6):
            share(a, kind).wait_send()
    for k in range(count):

        @pl.when(x != c)
        def _():
            for m in range(3):
                swap(k, m).wait_send()
            back(k).wait_send()

        for d in range(nz - 1):

            @pl.when((z >= d) & (z < nz - 1))
            def _():
                line(k, z - d, 0, d + 1).wait_send()

            @pl.when((z + d < nz) & (z > 0))
            def _():
                line(k, z + d, 1, d + 1).wait_send()

        for zs in range(nz):
            core_copy(k, zs).wait_send()
            pair_copy(k, zs).wait_send()

            @pl.when(zs != z)
            def _():
                passing(k, jnp.int32(zs), 0).wait_send()


def fused(n, cuts, gate, up, dn, late, early, cot, gain, sums, gain_sum):
    width, rows = gate.shape
    tokens, depth = late.shape
    nz, count = n // 2, len(cuts)
    most = max(size for _, size in cuts)
    vmem = pl.BlockSpec(memory_space=pltpu.VMEM)
    hbm = pl.BlockSpec(memory_space=pl.ANY)
    f32, bf16 = jnp.float32, jnp.bfloat16
    dma = pltpu.SemaphoreType.DMA
    crowd = 4 * tokens
    split = tokens * 3 // 128 * 16
    return pl.pallas_call(
        functools.partial(fused_kernel, n, cuts),
        out_shape=[jax.ShapeDtypeStruct((tokens, depth), bf16)] * 2
        + [jax.ShapeDtypeStruct((width, rows), f32)] * 3
        + [jax.ShapeDtypeStruct((1, depth), f32)],
        in_specs=[hbm] * 6 + [vmem] + [hbm] * 3 + [vmem],
        out_specs=[hbm] * 6,
        scratch_shapes=[
            pltpu.VMEM((3, width, depth), bf16),
            pltpu.VMEM((3, crowd, depth), bf16),
            pltpu.VMEM((tokens, depth), bf16),
            pltpu.VMEM((tokens, depth), bf16),
            pltpu.VMEM((3, width, rows), f32),
            pltpu.VMEM((3, width, depth), bf16),
            pltpu.VMEM((3, width, nz * rows), bf16),
            pltpu.VMEM((nz + 1, 3, width, rows), bf16),
            pltpu.VMEM((3, crowd, most), f32),
            pltpu.VMEM((3, width, crowd), bf16),
            pltpu.VMEM((crowd, width), bf16),
            pltpu.VMEM((crowd, width), bf16),
            pltpu.VMEM((crowd, width), bf16),
            pltpu.VMEM((2, crowd, depth), bf16),
            pltpu.VMEM((2, tokens, depth), bf16),
            pltpu.VMEM((2, tokens, depth), bf16),
            pltpu.VMEM((2, split, depth), bf16),
            pltpu.VMEM((2, tokens - split, depth), bf16),
            pltpu.VMEM((3, 1, depth), f32),
            pltpu.VMEM((3, 1, depth), f32),
            pltpu.VMEM((nz, 1, depth), f32),
            pltpu.VMEM((3, width, rows), bf16),
            pltpu.VMEM((3, width, rows), bf16),
            dma((count,)),
            dma((count,)),
            dma((6,)),
            dma((count, 3)),
            dma((count, 3)),
            dma((count, 3)),
            dma((count, 2, nz - 1)),
            dma((count, 2, nz - 1)),
            dma((count, nz)),
            dma((count, nz)),
            dma((3, 4)),
            dma((3, 4)),
            dma((count, nz)),
            dma((count, nz)),
            dma((count, nz)),
            dma((count, nz + 1)),
            dma((2, 6)),
            dma((2, 6)),
            dma((2 + nz,)),
            dma((2 + nz,)),
            dma((2,)),
            dma((count, 3)),
            dma(()),
            pltpu.VMEM((1, depth), f32),
        ],
        compiler_params=pltpu.CompilerParams(
            collective_id=2, has_side_effects=True, vmem_limit_bytes=FUSED_LIMIT
        ),
    )(gate, up, dn, late, early, cot, gain, *sums, gain_sum)


def settle_kernel(*refs):
    count = len(refs) // 3
    sources, targets, buffers = refs[:count], refs[count : 2 * count], refs[2 * count : 3 * count]
    in_sem, out_sem = refs[3 * count :]
    reads = [
        pltpu.make_async_copy(source, buffer, in_sem.at[k])
        for k, (source, buffer) in enumerate(zip(sources, buffers))
    ]
    writes = [
        pltpu.make_async_copy(buffer, target, out_sem.at[k])
        for k, (buffer, target) in enumerate(zip(buffers, targets))
    ]
    for copy in reads:
        copy.start()
    for read, write in zip(reads, writes):
        read.wait()
        write.start()
    for copy in writes:
        copy.wait()


def settle(arrays):
    hbm = pl.BlockSpec(memory_space=pl.ANY)
    return pl.pallas_call(
        settle_kernel,
        out_shape=[jax.ShapeDtypeStruct(array.shape, array.dtype) for array in arrays],
        in_specs=[hbm] * len(arrays),
        out_specs=[hbm] * len(arrays),
        scratch_shapes=[pltpu.VMEM(array.shape, array.dtype) for array in arrays]
        + [pltpu.SemaphoreType.DMA((len(arrays),))] * 2,
        compiler_params=pltpu.CompilerParams(vmem_limit_bytes=VMEM_LIMIT),
    )(*arrays)


def cut_hidden(width):
    step = -(-width // 384) * 128
    return tuple((at, min(step, width - at)) for at in range(0, width, step))


def per_device_fused(n, args):
    late, norm_gain, gate, up, dn, early, cot, gate_sum, up_sum, dn_sum, gain_sum = args
    depth = late.shape[1]
    out = fused(
        n,
        cut_hidden(gate.shape[1]),
        gate.T,
        up.T,
        dn.T,
        late,
        early,
        cot,
        norm_gain,
        (gate_sum.T, up_sum.T, dn_sum.T),
        gain_sum.reshape(1, depth),
    )
    late_out, early_grad, gate_out, up_out, dn_out, gain_out = settle(out)
    return late_out, early_grad, gate_out.T, up_out.T, dn_out.T, gain_out.reshape(depth)


def per_device(n, n_tp, *args):
    if n == 8 and n_tp == 4 and len(cut_hidden(args[2].shape[1])) == 3 and args[2].shape[0] % 128 == 0:
        return per_device_fused(n, args)
    return per_device_rings(n, n_tp, *args)


def solution(mesh):
    token = P(("fs", "tp"), None)
    weight = P("fs", "tp")
    return jax.shard_map(
        functools.partial(per_device, mesh.shape["fs"], mesh.shape["tp"]),
        mesh=mesh,
        in_specs=(token, P(), weight, weight, weight, token, token, weight, weight, weight, P()),
        out_specs=(token, token, weight, weight, weight, P()),
        check_vma=False,
    )
```

```python
import functools

import jax
import jax.numpy as jnp
from jax import lax
from jax.experimental import pallas as pl
from jax.experimental.pallas import tpu as pltpu
from jax.sharding import PartitionSpec as P

epsilon = 1e-05
MESH = pl.DeviceIdType.MESH
VMEM_LIMIT = 60 * 1024 * 1024
FUSED_LIMIT = 63 * 1024 * 1024


def ring_place(index, n):
    odd = lax.rem(index, 2)
    half = index // 2
    return (1 - odd) * half + odd * (n - 1 - half)


def ring_index(place, n):
    back = place // (n // 2)
    return (1 - back) * (2 * place) + back * (2 * (n - 1 - place) + 1)


def neighbours(n):
    place = ring_place(lax.axis_index("fs"), n)
    right = ring_index(lax.rem(place + 1, n), n)
    left = ring_index(lax.rem(place + n - 1, n), n)
    return place, right, left


def greet(n_tp, right, left):
    me_tp = lax.axis_index("tp")
    barrier = pltpu.get_barrier_semaphore()
    for target in (right, left):
        pl.semaphore_signal(barrier, inc=1, device_id=(target, me_tp), device_id_type=MESH)
    for away in range(1, n_tp):
        peer = lax.rem(me_tp + away, n_tp)
        pl.semaphore_signal(
            barrier, inc=1, device_id=(lax.axis_index("fs"), peer), device_id_type=MESH
        )
    pl.semaphore_wait(barrier, 2 + n_tp - 1)


def gather_kernel(n, n_tp, turned, *refs):
    gate_in, up_in, dn_in, late_in, early_in, cot_ref, gain_ref = refs[:7]
    gu_out, dn_out, late_all, early_out, cot_out, both_out, hid_out = refs[7:14]
    gate_buf, up_buf, gu_ref, dn_buf, dn_ref, late_buf, early_buf, late_ref = refs[14:22]
    gu_all, dn_all, early_all, cot_all, sum_gu, sum_dn = refs[22:28]
    send_sem, recv_sem, tp_send, tp_recv, own_sem, in_sem, out_sem = refs[28:]
    me_fs, me_tp = lax.axis_index("fs"), lax.axis_index("tp")
    tokens = late_in.shape[0]
    mine = pl.ds(pl.multiple_of(me_tp * tokens, tokens), tokens)
    rows, width = dn_ref.shape
    loads = [
        pltpu.make_async_copy(source, target, in_sem.at[k])
        for k, (source, target) in enumerate(
            (
                (gate_in, gate_buf),
                (up_in, up_buf),
                (early_in, early_buf),
                (late_in, late_buf),
                (dn_in, dn_buf),
                (cot_ref, cot_all.at[mine]),
            )
        )
    ]
    for copy in loads:
        copy.start()
    place, right, left = neighbours(n)
    greet(n_tp, right, left)
    half = rows // 2
    outs = (gu_out, dn_out)
    pairs = ((gu_ref, gu_all), (dn_ref, dn_all))

    def window(owner, way):
        return pl.ds(pl.multiple_of(owner * rows + way * half, half), half)

    def piece(step, c, way, first):
        block, whole = pairs[c]
        if way == 0:
            owner = ring_index(lax.rem(place - step + n, n), n)
            target = right
        else:
            owner = ring_index(lax.rem(place + step, n), n)
            target = left
        spot = whole.at[window(owner, way)]
        source = block.at[pl.ds(way * half, half)] if first else spot
        return pltpu.make_async_remote_copy(
            src_ref=source,
            dst_ref=spot,
            send_sem=send_sem.at[step, c, way],
            recv_sem=recv_sem.at[step, c, way],
            device_id=(target, me_tp),
            device_id_type=MESH,
        )

    token_pairs = (
        (early_all.at[mine], early_all),
        (cot_ref, cot_all),
        (late_ref, late_all),
    )

    def token_piece(a, away):
        block, whole = token_pairs[a]
        return pltpu.make_async_remote_copy(
            src_ref=block,
            dst_ref=whole.at[mine],
            send_sem=tp_send.at[a, away - 1],
            recv_sem=tp_recv.at[a, away - 1],
            device_id=(me_fs, lax.rem(me_tp + away, n_tp)),
            device_id_type=MESH,
        )

    def spread(a):
        for away in range(1, n_tp):
            token_piece(a, away).start()

    def arrived(a):
        for away in range(1, n_tp):
            token_piece(a, away).wait()

    def owner_of(step, way):
        if way == 0:
            return ring_index(lax.rem(place - step + n, n), n)
        return ring_index(lax.rem(place + step, n), n)

    def landed(step, c, way):
        some = window(owner_of(step + 1, way), way)
        return pltpu.make_async_copy(
            pairs[c][1].at[some], outs[c].at[some], out_sem.at[step, c, way]
        )

    totals = ((sum_gu, early_all), (sum_dn, cot_all))

    def add_rows(step, c):
        total, left = totals[c]
        for way in range(2):
            some = window(owner_of(step, way), way)
            total[...] += jnp.dot(
                left[:, some], pairs[c][1][some, :], preferred_element_type=jnp.float32
            )

    def norm(source, target, base):
        def part(k, carry):
            some = pl.ds(pl.multiple_of(k * 16, 16), 16)
            values = source[some, :].astype(jnp.float32)
            scale = lax.rsqrt(jnp.mean(values * values, axis=-1, keepdims=True) + epsilon)
            target[pl.ds(pl.multiple_of(base + k * 16, 16), 16), :] = (values * scale * gain_ref[...]).astype(jnp.bfloat16)
            return carry

        lax.fori_loop(0, tokens // 16, part, 0)

    def plain(buffer):
        return buffer[...].T if turned else buffer[...]

    loads[4].wait()
    dn_ref[...] = plain(dn_buf)
    for way in range(2):
        piece(0, 1, way, True).start()
    loads[0].wait()
    loads[1].wait()
    gu_ref[:, :width] = plain(gate_buf)
    gu_ref[:, width:] = plain(up_buf)
    for way in range(2):
        piece(0, 0, way, True).start()
    loads[2].wait()
    norm(early_buf, early_all, me_tp * tokens)
    spread(0)
    spread(1)
    loads[3].wait()
    norm(late_buf, late_ref, 0)
    spread(2)
    loads[5].wait()
    here = pl.ds(pl.multiple_of(me_fs * rows, rows), rows)
    gu_all[here, :] = gu_ref[...]
    dn_all[here, :] = dn_ref[...]
    sum_gu[...] = jnp.zeros_like(sum_gu)
    sum_dn[...] = jnp.zeros_like(sum_dn)
    own = [
        pltpu.make_async_copy(late_ref, late_all.at[mine], own_sem.at[0]),
        pltpu.make_async_copy(gu_ref, gu_out.at[here], own_sem.at[1]),
        pltpu.make_async_copy(dn_ref, dn_out.at[here], own_sem.at[2]),
    ]
    for copy in own:
        copy.start()
    keep = [
        pltpu.make_async_copy(early_all, early_out, own_sem.at[3]),
        pltpu.make_async_copy(cot_all, cot_out, own_sem.at[4]),
    ]

    def body(step, carry):
        for c in (1, 0):
            for way in range(2):
                piece(step - 1, c, way, False).wait_recv()
                piece(step, c, way, False).start()
                landed(step - 1, c, way).start()
            which = 1 - c

            @pl.when(step == n // 2)
            def _():
                arrived(which)
                keep[which].start()

            if turned:

                @pl.when(step >= n // 2)
                def _():
                    add_rows(2 * (step - n // 2), which)
                    add_rows(2 * (step - n // 2) + 1, which)

        return carry

    lax.fori_loop(1, n - 1, body, 0)
    if turned:
        for c in (1, 0):
            add_rows(n - 2, c)
    for c in (1, 0):
        for way in range(2):
            piece(n - 2, c, way, False).wait_recv()
            landed(n - 2, c, way).start()
            piece(0, c, way, True).wait_send()
        if turned:
            add_rows(n - 1, c)
        else:
            total, rest = totals[c]
            total[...] = jnp.dot(
                rest[...], pairs[c][1][...], preferred_element_type=jnp.float32
            )

    def finish(k, carry):
        some = pl.ds(pl.multiple_of(k * 64, 64), 64)
        gate, upper = sum_gu[some, :width], sum_gu[some, width:]
        sigma = 1.0 / (1.0 + jnp.exp(-gate))
        d_hidden = 0.5 * sum_dn[some, :]
        hid_out[some, :] = (gate * sigma * upper).astype(jnp.bfloat16)
        both_out[some, :width] = (
            d_hidden * upper * sigma * (1.0 + gate * (1.0 - sigma))
        ).astype(jnp.bfloat16)
        both_out[some, width:] = (d_hidden * gate * sigma).astype(jnp.bfloat16)
        return carry

    lax.fori_loop(0, n_tp * tokens // 64, finish, 0)

    def drain(step, carry):
        for c in (1, 0):
            for way in range(2):
                piece(step, c, way, False).wait_send()
        return carry

    lax.fori_loop(1, n - 1, drain, 0)

    def put(step, carry):
        for c in range(2):
            for way in range(2):
                landed(step, c, way).wait()
        return carry

    lax.fori_loop(0, n - 1, put, 0)
    for copy in own + keep:
        copy.wait()
    arrived(2)


def gather(n, n_tp, turned, gate, up, dn, late, early, cot, gain):
    rows, width = gate.shape[::-1] if turned else gate.shape
    tokens, depth = late.shape
    vmem = pl.BlockSpec(memory_space=pltpu.VMEM)
    hbm = pl.BlockSpec(memory_space=pl.ANY)
    bf16 = jnp.bfloat16
    return pl.pallas_call(
        functools.partial(gather_kernel, n, n_tp, turned),
        out_shape=[
            jax.ShapeDtypeStruct((n * rows, 2 * width), bf16),
            jax.ShapeDtypeStruct((n * rows, width), bf16),
        ]
        + [jax.ShapeDtypeStruct((n_tp * tokens, depth), bf16)] * 3
        + [
            jax.ShapeDtypeStruct((n_tp * tokens, 2 * width), bf16),
            jax.ShapeDtypeStruct((n_tp * tokens, width), bf16),
        ],
        in_specs=[hbm] * 6 + [vmem],
        out_specs=[hbm] * 5 + [vmem] * 2,
        scratch_shapes=[
            pltpu.VMEM(gate.shape, bf16),
            pltpu.VMEM(gate.shape, bf16),
            pltpu.VMEM((rows, 2 * width), bf16),
            pltpu.VMEM(gate.shape, bf16),
            pltpu.VMEM((rows, width), bf16),
        ]
        + [pltpu.VMEM((tokens, depth), bf16)] * 3
        + [
            pltpu.VMEM((n * rows, 2 * width), bf16),
            pltpu.VMEM((n * rows, width), bf16),
            pltpu.VMEM((n_tp * tokens, depth), bf16),
            pltpu.VMEM((n_tp * tokens, depth), bf16),
            pltpu.VMEM((n_tp * tokens, 2 * width), jnp.float32),
            pltpu.VMEM((n_tp * tokens, width), jnp.float32),
        ]
        + [
            pltpu.SemaphoreType.DMA((n - 1, 2, 2)),
            pltpu.SemaphoreType.DMA((n - 1, 2, 2)),
            pltpu.SemaphoreType.DMA((3, n_tp - 1)),
            pltpu.SemaphoreType.DMA((3, n_tp - 1)),
            pltpu.SemaphoreType.DMA((5,)),
            pltpu.SemaphoreType.DMA((6,)),
            pltpu.SemaphoreType.DMA((n - 1, 2, 2)),
        ],
        compiler_params=pltpu.CompilerParams(
            collective_id=0, has_side_effects=True, vmem_limit_bytes=VMEM_LIMIT
        ),
    )(gate, up, dn, late, early, cot, gain)


def reduce_kernel(n, n_tp, turned, *refs):
    early_side, cot_side, both_ref, hid_ref, gain_ref, early_all, gu_in, dn_in, late_in = refs[:9]
    gu_out, dn_out, mix_out, dnorm_out, gain_out = refs[9:14]
    gu_slots, dn_slots, gain_slots, gain_tp, gu_first, dn_first = refs[14:20]
    gu_all, dn_all, late_all, mix_ref, dnorm_ref, gain_sum = refs[20:26]
    send_sem, recv_sem, gain_send, gain_recv, tp_send, tp_recv, last_send, last_recv = refs[26:34]
    in_sem, own_sem = refs[34:]
    loads = [
        pltpu.make_async_copy(source, target, in_sem.at[k])
        for k, (source, target) in enumerate(
            ((gu_in, gu_all), (late_in, late_all), (dn_in, dn_all))
        )
    ]
    for copy in loads:
        copy.start()
    me_fs, me_tp = lax.axis_index("fs"), lax.axis_index("tp")
    place, right, left = neighbours(n)
    barrier = pltpu.get_barrier_semaphore()

    def greet_fs(away, carry):
        target = lax.rem(me_fs + away, n)
        pl.semaphore_signal(barrier, inc=1, device_id=(target, me_tp), device_id_type=MESH)
        return carry

    lax.fori_loop(1, n, greet_fs, 0)
    for away in range(1, n_tp):
        peer = lax.rem(me_tp + away, n_tp)
        pl.semaphore_signal(barrier, inc=1, device_id=(me_fs, peer), device_id_type=MESH)
    pl.semaphore_wait(barrier, n - 1 + n_tp - 1)
    width = dn_all.shape[1]
    half = gu_first.shape[1]
    rows = 2 * half
    tokens = late_all.shape[0] // n_tp
    sets = ((gu_first, gu_slots), (dn_first, dn_slots))
    factors = ((early_side, both_ref, 1.0), (cot_side, hid_ref, 0.5))

    def local(step, way):
        if way == 0:
            owner = ring_index(lax.rem(place - step - 1 + n, n), n)
        else:
            owner = ring_index(lax.rem(place + step + 1, n), n)
        return pl.ds(pl.multiple_of(owner * rows + way * half, half), half)

    def product(step, c, way):
        side, other, factor = factors[c]
        if turned:
            left, contract = side[:, local(step, way)], 0
        else:
            left, contract = side[local(step, way), :], 1
        return factor * lax.dot_general(
            left,
            other[...],
            (((contract,), (0,)), ((), ())),
            preferred_element_type=jnp.float32,
        )

    def piece(step, c, way, first, landed=False):
        start, slots = sets[c]
        source = start.at[way] if first else slots.at[way, step if landed else step - 1]
        return pltpu.make_async_remote_copy(
            src_ref=source,
            dst_ref=slots.at[way, step],
            send_sem=send_sem.at[step, c, way],
            recv_sem=recv_sem.at[step, c, way],
            device_id=((left if way else right), me_tp),
            device_id_type=MESH,
        )

    def gain_piece(away):
        return pltpu.make_async_remote_copy(
            src_ref=gain_slots.at[me_fs],
            dst_ref=gain_slots.at[me_fs],
            send_sem=gain_send.at[away - 1],
            recv_sem=gain_recv.at[away - 1],
            device_id=(lax.rem(me_fs + away, n), me_tp),
            device_id_type=MESH,
        )

    results = ((dnorm_ref, dnorm_out), (mix_ref, mix_out))

    def share(a, away):
        source, target = results[a]
        return pltpu.make_async_remote_copy(
            src_ref=source.at[away - 1],
            dst_ref=target.at[away - 1],
            send_sem=tp_send.at[a, away - 1],
            recv_sem=tp_recv.at[a, away - 1],
            device_id=(me_fs, lax.rem(me_tp + away, n_tp)),
            device_id_type=MESH,
        )

    def keep(a):
        source, target = results[a]
        return pltpu.make_async_copy(source.at[n_tp - 1], target.at[n_tp - 1], own_sem.at[a])

    def block_of(away):
        return pl.ds(pl.multiple_of(lax.rem(me_tp + away, n_tp) * tokens, tokens), tokens)

    def grad_block(away):
        some = block_of(away)
        part = lax.dot_general(
            both_ref[some, :],
            gu_all[...],
            (((1,), (1,)), ((), ())),
            preferred_element_type=jnp.float32,
        ).astype(jnp.bfloat16)
        dnorm_ref[away - 1] = part
        gain_sum[...] += jnp.sum(
            part.astype(jnp.float32) * early_all[some, :].astype(jnp.float32),
            axis=0,
            keepdims=True,
        )

    def late_block(away):
        both = jnp.dot(
            late_all[block_of(away), :], gu_all[...], preferred_element_type=jnp.float32
        )
        gate = both[:, :width]
        hidden = (gate / (1.0 + jnp.exp(-gate)) * both[:, width:]).astype(jnp.bfloat16)
        mix_ref[away - 1] = lax.dot_general(
            hidden, dn_all[...], (((1,), (1,)), ((), ())), preferred_element_type=jnp.float32
        ).astype(jnp.bfloat16)

    for c in range(2):
        for way in range(2):
            sets[c][0][way] = product(0, c, way).astype(jnp.bfloat16)
            piece(0, c, way, True).start()
    gain_sum[...] = jnp.zeros_like(gain_sum)
    for copy in loads:
        copy.wait()

    for c in range(2):
        (grad_block, late_block)[c](1)
        share(c, 1).start()

    def body(step, carry):
        for c in range(2):
            slots = sets[c][1]
            for way in range(2):
                term = product(step, c, way)
                piece(step - 1, c, way, False, True).wait_recv()
                slots[way, step - 1] = (
                    slots[way, step - 1].astype(jnp.float32) + term
                ).astype(jnp.bfloat16)
                piece(step, c, way, False).start()

            @pl.when(step < n_tp)
            def _():
                (grad_block, late_block)[c](step + 1)

            @pl.when(step < n_tp - 1)
            def _():
                share(c, step + 1).start()

            @pl.when(step == n_tp - 1)
            def _():
                keep(c).start()

        @pl.when(step == n_tp - 1)
        def _():
            gain_slots[me_fs] = gain_sum[...] / gain_ref[...]

            def send(away, inner):
                gain_piece(away).start()
                return inner

            lax.fori_loop(1, n, send, 0)

        return carry

    lax.fori_loop(1, n - 1, body, 0)

    def settle(away, inner):
        gain_piece(away).wait()
        return inner

    lax.fori_loop(1, n, settle, 0)
    gain_tp[me_tp] = lax.fori_loop(
        1, n, lambda k, total: total + gain_slots[k], gain_slots[0]
    )
    last = []
    for away in range(1, n_tp):
        peer = lax.rem(me_tp + away, n_tp)
        copy = pltpu.make_async_remote_copy(
            src_ref=gain_tp.at[me_tp],
            dst_ref=gain_tp.at[me_tp],
            send_sem=last_send.at[away - 1],
            recv_sem=last_recv.at[away - 1],
            device_id=(me_fs, peer),
            device_id_type=MESH,
        )
        copy.start()
        last.append(copy)
    for c in range(2):
        slots = sets[c][1]
        for way in range(2):
            term = product(n - 1, c, way)
            piece(n - 2, c, way, False, True).wait_recv()
            total = slots[way, n - 2].astype(jnp.float32) + term
            out = (gu_out, dn_out)[c]
            if turned:
                out[:, pl.ds(way * half, half)] = total.T
            else:
                out[pl.ds(way * half, half), :] = total
            piece(0, c, way, True).wait_send()
    for copy in last:
        copy.wait()
    total = gain_tp[0]
    for k in range(1, n_tp):
        total = total + gain_tp[k]
    gain_out[...] = total

    def drain(step, carry):
        for c in range(2):
            for way in range(2):
                piece(step, c, way, False).wait_send()
        return carry

    lax.fori_loop(1, n - 1, drain, 0)
    for a in range(2):
        keep(a).wait()
        for away in range(1, n_tp):
            share(a, away).wait()


def reduce(n, n_tp, turned, early_side, cot_side, both, hid, gain, early_all, gu_all, dn_all, late_all):
    rows = gu_all.shape[0] // n
    half = rows // 2
    width = dn_all.shape[1]
    shapes = [(rows, 2 * width), (rows, width)]
    if turned:
        shapes = [shape[::-1] for shape in shapes]
    depth = late_all.shape[1]
    tokens = late_all.shape[0] // n_tp
    vmem = pl.BlockSpec(memory_space=pltpu.VMEM)
    hbm = pl.BlockSpec(memory_space=pl.ANY)
    f32, bf16 = jnp.float32, jnp.bfloat16
    return pl.pallas_call(
        functools.partial(reduce_kernel, n, n_tp, turned),
        out_shape=[
            jax.ShapeDtypeStruct(shapes[0], f32),
            jax.ShapeDtypeStruct(shapes[1], f32),
            jax.ShapeDtypeStruct((n_tp, tokens, depth), bf16),
            jax.ShapeDtypeStruct((n_tp, tokens, depth), bf16),
            jax.ShapeDtypeStruct(gain.shape, f32),
        ],
        in_specs=[vmem] * 6 + [hbm] * 3,
        out_specs=[vmem, vmem, hbm, hbm, vmem],
        scratch_shapes=[
            pltpu.VMEM((2, n - 1, half, 2 * width), bf16),
            pltpu.VMEM((2, n - 1, half, width), bf16),
            pltpu.VMEM((n,) + gain.shape, f32),
            pltpu.VMEM((n_tp,) + gain.shape, f32),
            pltpu.VMEM((2, half, 2 * width), bf16),
            pltpu.VMEM((2, half, width), bf16),
            pltpu.VMEM(gu_all.shape, bf16),
            pltpu.VMEM(dn_all.shape, bf16),
            pltpu.VMEM(late_all.shape, bf16),
            pltpu.VMEM((n_tp, tokens, depth), bf16),
            pltpu.VMEM((n_tp, tokens, depth), bf16),
            pltpu.VMEM(gain.shape, f32),
            pltpu.SemaphoreType.DMA((n - 1, 2, 2)),
            pltpu.SemaphoreType.DMA((n - 1, 2, 2)),
            pltpu.SemaphoreType.DMA((n - 1,)),
            pltpu.SemaphoreType.DMA((n - 1,)),
            pltpu.SemaphoreType.DMA((2, n_tp - 1)),
            pltpu.SemaphoreType.DMA((2, n_tp - 1)),
            pltpu.SemaphoreType.DMA((n_tp - 1,)),
            pltpu.SemaphoreType.DMA((n_tp - 1,)),
            pltpu.SemaphoreType.DMA((3,)),
            pltpu.SemaphoreType.DMA((2,)),
        ],
        compiler_params=pltpu.CompilerParams(
            collective_id=1, has_side_effects=True, vmem_limit_bytes=VMEM_LIMIT
        ),
    )(early_side, cot_side, both, hid, gain, early_all, gu_all, dn_all, late_all)


def per_device_rings(
    n,
    n_tp,
    late_input,
    norm_gain,
    gate_weight,
    up_weight,
    down_weight,
    early_input,
    cotangent,
    gate_sum,
    up_sum,
    down_sum,
    gain_sum,
):
    gain_f = norm_gain.astype(jnp.float32)
    width = gate_weight.shape[1]
    depth = late_input.shape[1]
    turned = gate_weight.shape[0] % 256 == 0
    weights = [gate_weight, up_weight, down_weight]
    if turned:
        weights = [weight.T for weight in weights]
    gain_row = gain_f.reshape(1, depth)
    gu_all, down_all, late_all, early_all, cot_all, d_both, hidden_e = gather(
        n, n_tp, turned, *weights, late_input, early_input, cotangent, gain_row
    )
    sides = (early_all, cot_all) if turned else (early_all.T, cot_all.T)
    gu_grad, down_grad, mix_got, d_got, gain_total = reduce(
        n, n_tp, turned, *sides, d_both, hidden_e, gain_row, early_all, gu_all, down_all, late_all
    )
    if turned:
        gate_grad, up_grad, down_grad = gu_grad[:width].T, gu_grad[width:].T, down_grad.T
    else:
        gate_grad, up_grad = gu_grad[:, :width], gu_grad[:, width:]

    def gathered(got):
        total = got[0].astype(jnp.float32)
        for k in range(1, n_tp):
            total = total + got[k].astype(jnp.float32)
        return total

    values = late_input.astype(jnp.float32)
    values_e = early_input.astype(jnp.float32)
    scale_e = lax.rsqrt(jnp.mean(values_e * values_e, axis=-1, keepdims=True) + epsilon)
    late_out = (values + 0.5 * gathered(mix_got)).astype(jnp.bfloat16)
    scaled_grad = gathered(d_got) * gain_f
    early_grad = (
        cotangent.astype(jnp.float32)
        + scale_e * scaled_grad
        - values_e * scale_e**3 * jnp.mean(values_e * scaled_grad, axis=-1, keepdims=True)
    ).astype(jnp.bfloat16)
    return (
        late_out,
        early_grad,
        gate_sum + gate_grad,
        up_sum + up_grad,
        down_sum + down_grad,
        gain_sum + gain_total.reshape(depth),
    )


def fused_kernel(n, cuts, *refs):
    gate_in, up_in, dn_in, late_in, early_in, cot_in, gain_ref = refs[:7]
    sums_in, gain_sum_ref = refs[7:10], refs[10]
    token_outs, sum_outs, gain_out = refs[11:13], refs[13:16], refs[16]
    wall, toks, early_raw, late_raw, sums, grad, pair, slots = refs[17:25]
    act_f, act_t, d_gate, d_up, hid_l, part = refs[25:31]
    from_x, from_y, diag_x, diag_y, gain_mine, gain_got, gain_z = refs[31:38]
    back_mine, back_got, back_send, back_recv = refs[38:42]
    token_sem, sum_sem, gain_sem, gain_f = refs[-4:]
    load_sem, own_sem, swap_send, swap_recv, line_send, line_recv = refs[42:48]
    core_send, core_recv, tok_send, tok_recv, pair_send, pair_recv = refs[48:54]
    rs_send, rs_recv, xy_send, xy_recv, gain_send, gain_recv = refs[54:-4]
    nz = n // 2
    fs, tp = lax.axis_index("fs"), lax.axis_index("tp")
    z, x = fs // 2, lax.rem(fs, 2)
    y, c = tp // 2, lax.rem(tp, 2)
    weights = (gate_in, up_in, dn_in)
    tokens, depth = late_in.shape
    width, rows = gate_in.shape
    split = tokens // 64 * 16
    tok_splits = (16, tokens // 2, tokens // 2)
    bf16, f32 = jnp.bfloat16, jnp.float32
    count = len(cuts)
    straight = x == c

    def at(z_at, x_at, y_at, c_at):
        return (2 * z_at + x_at, 2 * y_at + c_at)

    up_z, down_z = lax.rem(z + 1, nz), lax.rem(z + nz - 1, nz)
    partner = at(z, x, y, 1 - c)
    x_side = at(z, 1 - x, y, c)
    y_side = at(z, x, 1 - y, c)
    crossed = at(z, c, y, x)

    def send(source, target, send_sem, recv_sem, device):
        return pltpu.make_async_remote_copy(
            src_ref=source,
            dst_ref=target,
            send_sem=send_sem,
            recv_sem=recv_sem,
            device_id=device,
            device_id_type=MESH,
        )

    def hold(k):
        return pl.ds(cuts[k][0], cuts[k][1])

    def block(j, wide=1):
        return pl.ds(pl.multiple_of(j * rows, rows), wide * rows)

    def some(start, size):
        return pl.ds(pl.multiple_of(start, 16), size)

    def own_load(k, m):
        return pltpu.make_async_copy(
            weights[m].at[hold(k)], wall.at[m, hold(k), block(fs)], own_sem.at[k, m]
        )

    def swap(k, m):
        return send(
            weights[m].at[hold(k)],
            wall.at[m, hold(k), block(fs)],
            swap_send.at[k, m],
            swap_recv.at[k, m],
            crossed,
        )

    p_me, p_x, p_y = 2 * x + y, 2 * (1 - x) + y, 2 * x + 1 - y
    p_d = 3 - p_me

    def place(p, start=0, size=tokens):
        return some(p * tokens + start, size)

    loads = [
        pltpu.make_async_copy(source, target, load_sem.at[i])
        for i, (source, target) in enumerate(
            (
                (early_in, early_raw),
                (late_in, late_raw),
                (cot_in, toks.at[1, place(p_me)]),
                (sums_in[0], sums.at[0]),
                (sums_in[1], sums.at[1]),
                (sums_in[2], sums.at[2]),
            )
        )
    ]
    for copy in loads[:3]:
        copy.start()

    @pl.when(straight)
    def _():
        for k in range(count):
            for m in range(3):
                own_load(k, m).start()

    for copy in loads[3:]:
        copy.start()

    barrier = pltpu.get_barrier_semaphore()

    def greet_at(device):
        pl.semaphore_signal(barrier, inc=1, device_id=device, device_id_type=MESH)

    for away in range(1, nz):
        greet_at(at(lax.rem(z + away, nz), x, y, c))
    for device in (partner, x_side, y_side):
        greet_at(device)

    @pl.when(x != c)
    def _():
        greet_at(crossed)

    def tok(a, kind):
        cut = tok_splits[a]
        if kind < 2:
            where = place(p_me)
        elif kind == 2:
            where = place(p_y, 0, cut)
        else:
            where = place(p_x, cut, tokens - cut)
        spot = toks.at[a, where]
        source = cot_in if a == 1 and kind < 2 else spot
        return send(
            source, spot, tok_send.at[a, kind], tok_recv.at[a, kind], y_side if kind % 2 else x_side
        )

    def tok_over_x(a):
        tok(a, 1).wait_recv()
        tok(a, 2).start()

    def tok_over_y(a):
        tok(a, 0).wait_recv()
        tok(a, 3).start()

    def tok_rest(a):
        tok(a, 2).wait_recv()
        tok(a, 3).wait_recv()

    def line(k, zs, way, dist):
        spot = wall.at[:, hold(k), block(2 * zs + c)]
        return send(
            spot,
            spot,
            line_send.at[k, way, dist - 1],
            line_recv.at[k, way, dist - 1],
            at(down_z if way else up_z, x, y, c),
        )

    def core_copy(k, zs):
        spot = wall.at[:, hold(k), block(2 * zs + c)]
        return send(spot, spot, core_send.at[k, zs], core_recv.at[k, zs], partner)

    def pump(k, d):
        if d == 0:

            @pl.when(straight)
            def _():
                for m in range(3):
                    own_load(k, m).wait()

            @pl.when(x != c)
            def _():
                for m in range(3):
                    swap(k, m).wait_recv()

            core_copy(k, z).start()
            return

        @pl.when(z >= d)
        def _():
            line(k, z - d, 0, d).wait_recv()

            if d < nz - 1:

                @pl.when(z < nz - 1)
                def _():
                    line(k, z - d, 0, d + 1).start()

            core_copy(k, z - d).start()

        @pl.when(z + d < nz)
        def _():
            line(k, z + d, 1, d).wait_recv()

            if d < nz - 1:

                @pl.when(z > 0)
                def _():
                    line(k, z + d, 1, d + 1).start()

            core_copy(k, z + d).start()

    def lead(k):
        pump(k, 0)

        @pl.when(z == 0)
        def _():
            line(k, z, 0, 1).start()

        @pl.when(z == nz - 1)
        def _():
            line(k, z, 1, 1).start()

    def follow(k):
        @pl.when((z < nz - 1) & (z > 0))
        def _():
            line(k, z, 0, 1).start()
            line(k, z, 1, 1).start()

    def weights_in(k):
        for zs in range(nz):
            core_copy(k, zs).wait_recv()

    def norm(source, a):
        def step(i, carry):
            values = source[some(i * 16, 16), :].astype(f32)
            scale = lax.rsqrt(jnp.mean(values * values, axis=-1, keepdims=True) + epsilon)
            toks[a, some(p_me * tokens + i * 16, 16), :] = (
                values * scale * gain_f[...]
            ).astype(bf16)
            return carry

        lax.fori_loop(0, tokens // 16, step, 0)

    def dot(left, right, sides):
        return lax.dot_general(left, right, (sides, ((), ())), preferred_element_type=f32)

    def hidden_dots(k, triples):
        size = cuts[k][1]
        for i, a, m in triples:
            act_f[i, :, :size] = dot(toks[a], wall[m, hold(k), :], ((1,), (1,)))

    def act_first(k):
        hidden_dots(k, ((0, 0, 0), (1, 0, 1)))

    def act_second(k):
        size = cuts[k][1]
        hidden_dots(k, ((2, 1, 2),))

        def step(i, carry):
            part_of = pl.ds(pl.multiple_of(i * 128, 128), 128)
            gate, upper = act_f[0, part_of, :size], act_f[1, part_of, :size]
            sigma = 1.0 / (1.0 + jnp.exp(-gate))
            d_hidden = 0.5 * act_f[2, part_of, :size]
            hidden = (gate * sigma * upper).astype(bf16)
            dg = (d_hidden * upper * sigma * (1.0 + gate * (1.0 - sigma))).astype(bf16)
            du = (d_hidden * gate * sigma).astype(bf16)
            d_gate[part_of, hold(k)] = dg
            d_up[part_of, hold(k)] = du
            act_t[0, hold(k), part_of] = dg.T
            act_t[1, hold(k), part_of] = du.T
            act_t[2, hold(k), part_of] = hidden.T
            return carry

        lax.fori_loop(0, 4 * tokens // 128, step, 0)

    def act_late(k):
        size = cuts[k][1]
        hidden_dots(k, ((0, 2, 0), (1, 2, 1)))

        def step(i, carry):
            part_of = pl.ds(pl.multiple_of(i * 64, 64), 64)
            gate, upper = act_f[0, part_of, :size], act_f[1, part_of, :size]
            hid_l[part_of, hold(k)] = (gate / (1.0 + jnp.exp(-gate)) * upper).astype(bf16)
            return carry

        lax.fori_loop(0, 4 * tokens // 64, step, 0)

    def turn(i):
        near = (1 - lax.rem(i, 2)) * (nz - 1 - i // 2) + lax.rem(i, 2) * (i // 2)
        far = (z >= nz // 2).astype(jnp.int32)
        return (1 - far) * near + far * (nz - 1 - near)

    def pair_copy(k, zq):
        return send(
            grad.at[:, hold(k), block(2 * zq + 1 - c)],
            pair.at[:, hold(k), block(zq)],
            pair_send.at[k, zq],
            pair_recv.at[k, zq],
            partner,
        )

    def products(k):
        def step(i, carry):
            zq = turn(i)
            both = block(2 * zq, 2)
            gains = jnp.zeros((1, 2 * rows), f32)
            for m in range(3):
                term = dot(act_t[m, hold(k), :], toks[m // 2, :, both], ((1,), (0,)))
                grad[m, hold(k), both] = term.astype(bf16)
                if m < 2:
                    gains += jnp.sum(
                        term * wall[m, hold(k), both].astype(f32), axis=0, keepdims=True
                    )
            pair_copy(k, zq).start()
            gain_mine[0, :, both] += gains
            return carry

        lax.fori_loop(0, nz, step, 0)

    def passing(k, zq, way):
        if way == 0:
            target, slot = up_z, zq
        else:
            last = (zq == z - 1).astype(jnp.int32)
            target, slot = down_z, last * nz + (1 - last) * zq
        return send(
            grad.at[:, hold(k), block(2 * zq + c)],
            slots.at[slot, :, hold(k), :],
            rs_send.at[k, zq],
            rs_recv.at[k, slot],
            at(target, x, y, c),
        )

    def landed(k, slot):
        here = slots.at[slot, :, hold(k), :]
        return send(here, here, rs_send.at[k, 0], rs_recv.at[k, slot], partner)

    def pass_on(k, zq):
        @pl.when(zq > z)
        def _():
            passing(k, zq, 0).start()

        @pl.when(zq < z)
        def _():
            passing(k, zq, 1).start()

    def upstream(zq):
        return ((zq > z) & (z > 0)) | ((zq < z) & (z < nz - 1))

    def combine_free(k, least=1, most=nz):
        def step(i, carry):
            zq = turn(i)
            away = jnp.abs(zq - z)

            @pl.when((away >= least) & (away <= most) & jnp.logical_not(upstream(zq)))
            def _():
                pair_copy(k, zq).wait_recv()
                for m in range(3):
                    spot = (m, hold(k), block(2 * zq + c))
                    grad[spot] = (
                        grad[spot].astype(f32) + pair[m, hold(k), block(zq)].astype(f32)
                    ).astype(bf16)
                pass_on(k, zq)

            return carry

        lax.fori_loop(0, nz, step, 0)

    def combine_up(k, i):
        zq = turn(jnp.int32(i))

        @pl.when((zq != z) & upstream(zq))
        def _():
            pair_copy(k, zq).wait_recv()
            landed(k, zq).wait_recv()
            for m in range(3):
                spot = (m, hold(k), block(2 * zq + c))
                grad[spot] = (
                    grad[spot].astype(f32)
                    + pair[m, hold(k), block(zq)].astype(f32)
                    + slots[zq, m, hold(k), :].astype(f32)
                ).astype(bf16)
            pass_on(k, zq)

    def back(k):
        spot = back_mine.at[:, hold(k), :]
        return send(
            spot, back_got.at[:, hold(k), :], back_send.at[k], back_recv.at[k], crossed
        )

    factors = (1.0, 1.0, 0.5)

    def put(k, m):
        return pltpu.make_async_copy(
            sums.at[m, hold(k), :], sum_outs[m].at[hold(k), :], sum_sem.at[k, m]
        )

    def put_tokens(a):
        return pltpu.make_async_copy((early_raw, late_raw)[a], token_outs[1 - a], token_sem.at[a])

    def finish(k):
        pair_copy(k, z).wait_recv()

        @pl.when(z > 0)
        def _():
            landed(k, z).wait_recv()

        @pl.when(z < nz - 1)
        def _():
            landed(k, nz).wait_recv()

        def total(m):
            return (
                grad[m, hold(k), block(2 * z + c)].astype(f32)
                + pair[m, hold(k), block(z)].astype(f32)
                + slots[z, m, hold(k), :].astype(f32)
                + slots[nz, m, hold(k), :].astype(f32)
            )

        @pl.when(straight)
        def _():
            for m in range(3):
                sums[m, hold(k), :] += factors[m] * total(m)
                put(k, m).start()

        @pl.when(x != c)
        def _():
            for m in range(3):
                back_mine[m, hold(k), :] = total(m).astype(bf16)
            back(k).start()

    def finish_back(k):
        @pl.when(x != c)
        def _():
            back(k).wait_recv()
            for m in range(3):
                sums[m, hold(k), :] += factors[m] * back_got[m, hold(k), :].astype(f32)
                put(k, m).start()

    low, high = (0, split), (split, tokens - split)

    def share(a, kind):
        def of(p, piece):
            return part.at[a, place(p, *piece)]

        source, target = (
            (of(p_d, low), diag_x.at[a]),
            (of(p_d, high), diag_y.at[a]),
            (of(p_x, low), from_x.at[a, pl.ds(*low)]),
            (of(p_y, high), from_y.at[a, pl.ds(*high)]),
            (of(p_x, high), from_x.at[a, pl.ds(*high)]),
            (of(p_y, low), from_y.at[a, pl.ds(*low)]),
        )[kind]
        device = (x_side, y_side, x_side, y_side, x_side, y_side)[kind]
        return send(source, target, xy_send.at[a, kind], xy_recv.at[a, kind], device)

    def half_of(side):
        return pl.ds(pl.multiple_of(side * 2 * tokens, 2 * tokens), 2 * tokens)

    def grad_half(side):
        where = half_of(side)
        both = (
            dot(d_gate[where, :], wall[0], ((1,), (0,)))
            + dot(d_up[where, :], wall[1], ((1,), (0,)))
        ).astype(bf16)
        part[0, where, :] = both

    def late_half(side):
        where = half_of(side)
        part[1, where, :] = dot(hid_l[where, :], wall[2], ((1,), (0,))).astype(bf16)

    def share_forward(a):
        share(a, 1).wait_recv()
        where = place(p_x, *high)
        part[a, where, :] = (part[a, where, :].astype(f32) + diag_y[a].astype(f32)).astype(bf16)
        share(a, 4).start()
        share(a, 0).wait_recv()
        where = place(p_y, *low)
        part[a, where, :] = (part[a, where, :].astype(f32) + diag_x[a].astype(f32)).astype(bf16)
        share(a, 5).start()

    def share_in(a):
        for kind in range(2, 6):
            share(a, kind).wait_recv()

    def own_total(a, i):
        where, mine = some(i * 16, 16), some(p_me * tokens + i * 16, 16)
        return (
            part[a, mine, :].astype(f32)
            + from_x[a, where, :].astype(f32)
            + from_y[a, where, :].astype(f32)
        )

    def write_late():
        def step(i, carry):
            where = some(i * 16, 16)
            late_raw[where, :] = (
                late_raw[where, :].astype(f32) + 0.5 * own_total(1, i)
            ).astype(bf16)
            return carry

        lax.fori_loop(0, tokens // 16, step, 0)

    def write_early():
        def step(i, carry):
            where = some(i * 16, 16)
            values = early_raw[where, :].astype(f32)
            scale = lax.rsqrt(jnp.mean(values * values, axis=-1, keepdims=True) + epsilon)
            scaled = own_total(0, i) * gain_f[...]
            mean = jnp.mean(values * scaled, axis=-1, keepdims=True)
            cot = toks[1, some(p_me * tokens + i * 16, 16), :].astype(f32)
            early_raw[where, :] = (cot + scale * scaled - values * scale**3 * mean).astype(bf16)
            return carry

        lax.fori_loop(0, tokens // 16, step, 0)

    def gain_step(i):
        return send(
            gain_mine.at[i],
            gain_got.at[i],
            gain_send.at[i],
            gain_recv.at[i],
            (partner, x_side, y_side)[i],
        )

    def gain_away(away):
        return send(
            gain_z.at[z],
            gain_z.at[z],
            gain_send.at[2 + away],
            gain_recv.at[2 + away],
            at(lax.rem(z + away, nz), x, y, c),
        )

    def gain_next(i):
        gain_step(i).wait_recv()
        total = gain_mine[i] + gain_got[i]
        if i < 2:
            gain_mine[i + 1] = total
            gain_step(i + 1).start()
        else:
            gain_z[z] = total
            for away in range(1, nz):
                gain_away(away).start()

    def each_step(steps):
        for step in steps:
            if step[1] == 0:
                lead(step[0])
                follow(step[0])
            elif step[1] < 0:
                (lead, follow)[step[1] + 2](step[0])
            else:
                pump(*step)

    def when_straight(*steps):
        @pl.when(straight)
        def _():
            each_step(steps)

    def when_crossed(*steps):
        @pl.when(x != c)
        def _():
            each_step(steps)

    inner = (z > 0) & (z < nz - 1)

    def when_straight_inner(*steps):
        @pl.when(straight & inner)
        def _():
            each_step(steps)

    def when_straight_outer(*steps):
        @pl.when(straight & jnp.logical_not(inner))
        def _():
            each_step(steps)

    def when_inner(*steps):
        @pl.when(inner)
        def _():
            each_step(steps)

    def when_outer(*steps):
        @pl.when(jnp.logical_not(inner))
        def _():
            each_step(steps)

    gain_f[...] = gain_ref[...].astype(f32).reshape(1, depth)
    loads[0].wait()
    norm(early_raw, 0)

    @pl.when(straight)
    def _():
        pl.semaphore_wait(barrier, nz - 1 + 3)

    @pl.when(x != c)
    def _():
        pl.semaphore_wait(barrier, nz - 1 + 4)

    @pl.when(x != c)
    def _():
        for k in range(2):
            for m in range(3):
                swap(k, m).start()

    for a in range(2):
        tok(a, 1).start()

    @pl.when(x != c)
    def _():
        for a in range(2):
            tok(a, 0).start()

    when_straight((0, 0), (1, -2))
    loads[1].wait()
    norm(late_raw, 2)
    gain_mine[0] = jnp.zeros((1, depth), f32)

    @pl.when(z == 0)
    def _():
        slots[0] = jnp.zeros_like(slots[0])

    @pl.when(z == nz - 1)
    def _():
        slots[nz] = jnp.zeros_like(slots[nz])

    when_crossed((0, 0))
    when_straight((0, 1))

    @pl.when(straight)
    def _():
        for a in range(2):
            tok(a, 0).start()

    tok_over_x(0)
    when_straight((2, -2), (0, 2), (1, -1))
    when_crossed((1, -2), (0, 1))
    tok_over_y(0)
    when_straight((0, 3), (1, 1))
    when_crossed((0, 2), (1, -1))
    loads[2].wait()
    tok_over_x(1)

    @pl.when(x != c)
    def _():
        for m in range(3):
            swap(2, m).start()

    tok_over_y(1)
    tok_rest(0)
    when_crossed((0, 3))
    weights_in(0)
    act_first(0)
    when_straight_inner((1, 2), (2, -1))
    tok_rest(1)

    @pl.when(straight)
    def _():
        tok(2, 1).start()
        tok(2, 0).start()

    act_second(0)
    products(0)
    when_crossed((2, -2))
    combine_free(0)

    @pl.when(x != c)
    def _():
        tok(2, 1).start()
        tok(2, 0).start()

    when_straight_outer((1, 2), (2, -1))
    when_crossed((1, 1), (1, 2), (2, -1))
    when_inner((2, 1))
    when_outer((1, 3))
    tok_over_x(2)
    tok_over_y(2)
    combine_up(0, 0)
    when_inner((2, 2))
    weights_in(1)
    act_first(1)
    act_second(1)
    products(1)
    combine_free(1, 2)
    combine_up(0, 1)
    when_outer((2, 1))
    tok_rest(2)
    act_late(0)
    when_outer((2, 2))
    act_late(1)
    combine_up(0, 2)
    combine_up(0, 3)
    when_outer((2, 3))
    weights_in(2)
    act_first(2)
    act_second(2)
    products(2)
    gain_mine[0] = gain_mine[0] / gain_f[...]
    gain_step(0).start()
    grad_half(1 - x)
    gain_next(0)
    for kind in range(3):
        share(0, kind).start()
    combine_free(2, 2)
    combine_free(1, 1, 1)
    combine_free(2, 1, 1)
    act_late(2)
    late_half(1 - x)
    gain_next(1)
    for kind in range(3):
        share(1, kind).start()
    for i in range(3):
        loads[3 + i].wait()
    finish(0)
    combine_up(1, 0)
    grad_half(x)
    share(0, 3).start()
    late_half(x)
    share(1, 3).start()
    combine_up(1, 1)
    combine_up(1, 2)
    share_forward(0)
    combine_up(2, 0)
    gain_next(2)
    combine_up(2, 2)
    share_forward(1)
    combine_up(2, 1)
    finish(1)
    finish(2)
    finish_back(0)
    share_in(0)
    write_early()
    put_tokens(0).start()
    share_in(1)
    write_late()
    put_tokens(1).start()
    for away in range(1, nz):
        gain_away(away).wait_recv()
    total = gain_z[0]
    for k in range(1, nz):
        total = total + gain_z[k]
    gain_got[2] = gain_sum_ref[...] + total
    put_gain = pltpu.make_async_copy(gain_got.at[2], gain_out, gain_sem)
    put_gain.start()
    finish_back(1)
    finish_back(2)

    put_gain.wait()
    for a in range(2):
        put_tokens(a).wait()
    for k in range(count):
        for m in range(3):
            put(k, m).wait()
    for i in range(3):
        gain_step(i).wait_send()
    for away in range(1, nz):
        gain_away(away).wait_send()
    for a in range(3):
        for kind in range(4):
            tok(a, kind).wait_send()
    for a in range(2):
        for kind in range(6):
            share(a, kind).wait_send()
    for k in range(count):

        @pl.when(x != c)
        def _():
            for m in range(3):
                swap(k, m).wait_send()
            back(k).wait_send()

        for d in range(nz - 1):

            @pl.when((z >= d) & (z < nz - 1))
            def _():
                line(k, z - d, 0, d + 1).wait_send()

            @pl.when((z + d < nz) & (z > 0))
            def _():
                line(k, z + d, 1, d + 1).wait_send()

        for zs in range(nz):
            core_copy(k, zs).wait_send()
            pair_copy(k, zs).wait_send()

            @pl.when(zs != z)
            def _():
                passing(k, jnp.int32(zs), 0).wait_send()


def fused(n, cuts, gate, up, dn, late, early, cot, gain, sums, gain_sum):
    width, rows = gate.shape
    tokens, depth = late.shape
    nz, count = n // 2, len(cuts)
    most = max(size for _, size in cuts)
    vmem = pl.BlockSpec(memory_space=pltpu.VMEM)
    hbm = pl.BlockSpec(memory_space=pl.ANY)
    f32, bf16 = jnp.float32, jnp.bfloat16
    dma = pltpu.SemaphoreType.DMA
    crowd = 4 * tokens
    split = tokens // 64 * 16
    return pl.pallas_call(
        functools.partial(fused_kernel, n, cuts),
        out_shape=[jax.ShapeDtypeStruct((tokens, depth), bf16)] * 2
        + [jax.ShapeDtypeStruct((width, rows), f32)] * 3
        + [jax.ShapeDtypeStruct((1, depth), f32)],
        in_specs=[hbm] * 6 + [vmem] + [hbm] * 3 + [vmem],
        out_specs=[hbm] * 6,
        scratch_shapes=[
            pltpu.VMEM((3, width, depth), bf16),
            pltpu.VMEM((3, crowd, depth), bf16),
            pltpu.VMEM((tokens, depth), bf16),
            pltpu.VMEM((tokens, depth), bf16),
            pltpu.VMEM((3, width, rows), f32),
            pltpu.VMEM((3, width, depth), bf16),
            pltpu.VMEM((3, width, nz * rows), bf16),
            pltpu.VMEM((nz + 1, 3, width, rows), bf16),
            pltpu.VMEM((3, crowd, most), f32),
            pltpu.VMEM((3, width, crowd), bf16),
            pltpu.VMEM((crowd, width), bf16),
            pltpu.VMEM((crowd, width), bf16),
            pltpu.VMEM((crowd, width), bf16),
            pltpu.VMEM((2, crowd, depth), bf16),
            pltpu.VMEM((2, tokens, depth), bf16),
            pltpu.VMEM((2, tokens, depth), bf16),
            pltpu.VMEM((2, split, depth), bf16),
            pltpu.VMEM((2, tokens - split, depth), bf16),
            pltpu.VMEM((3, 1, depth), f32),
            pltpu.VMEM((3, 1, depth), f32),
            pltpu.VMEM((nz, 1, depth), f32),
            pltpu.VMEM((3, width, rows), bf16),
            pltpu.VMEM((3, width, rows), bf16),
            dma((count,)),
            dma((count,)),
            dma((6,)),
            dma((count, 3)),
            dma((count, 3)),
            dma((count, 3)),
            dma((count, 2, nz - 1)),
            dma((count, 2, nz - 1)),
            dma((count, nz)),
            dma((count, nz)),
            dma((3, 4)),
            dma((3, 4)),
            dma((count, nz)),
            dma((count, nz)),
            dma((count, nz)),
            dma((count, nz + 1)),
            dma((2, 6)),
            dma((2, 6)),
            dma((2 + nz,)),
            dma((2 + nz,)),
            dma((2,)),
            dma((count, 3)),
            dma(()),
            pltpu.VMEM((1, depth), f32),
        ],
        compiler_params=pltpu.CompilerParams(
            collective_id=2, has_side_effects=True, vmem_limit_bytes=FUSED_LIMIT
        ),
    )(gate, up, dn, late, early, cot, gain, *sums, gain_sum)


def settle_kernel(*refs):
    count = len(refs) // 3
    sources, targets, buffers = refs[:count], refs[count : 2 * count], refs[2 * count : 3 * count]
    in_sem, out_sem = refs[3 * count :]
    reads = [
        pltpu.make_async_copy(source, buffer, in_sem.at[k])
        for k, (source, buffer) in enumerate(zip(sources, buffers))
    ]
    writes = [
        pltpu.make_async_copy(buffer, target, out_sem.at[k])
        for k, (buffer, target) in enumerate(zip(buffers, targets))
    ]
    for copy in reads:
        copy.start()
    for read, write in zip(reads, writes):
        read.wait()
        write.start()
    for copy in writes:
        copy.wait()


def settle(arrays):
    hbm = pl.BlockSpec(memory_space=pl.ANY)
    return pl.pallas_call(
        settle_kernel,
        out_shape=[jax.ShapeDtypeStruct(array.shape, array.dtype) for array in arrays],
        in_specs=[hbm] * len(arrays),
        out_specs=[hbm] * len(arrays),
        scratch_shapes=[pltpu.VMEM(array.shape, array.dtype) for array in arrays]
        + [pltpu.SemaphoreType.DMA((len(arrays),))] * 2,
        compiler_params=pltpu.CompilerParams(vmem_limit_bytes=VMEM_LIMIT),
    )(*arrays)


def cut_hidden(width):
    step = -(-width // 384) * 128
    return tuple((at, min(step, width - at)) for at in range(0, width, step))


def per_device_fused(n, args):
    late, norm_gain, gate, up, dn, early, cot, gate_sum, up_sum, dn_sum, gain_sum = args
    depth = late.shape[1]
    out = fused(
        n,
        cut_hidden(gate.shape[1]),
        gate.T,
        up.T,
        dn.T,
        late,
        early,
        cot,
        norm_gain,
        (gate_sum.T, up_sum.T, dn_sum.T),
        gain_sum.reshape(1, depth),
    )
    late_out, early_grad, gate_out, up_out, dn_out, gain_out = settle(out)
    return late_out, early_grad, gate_out.T, up_out.T, dn_out.T, gain_out.reshape(depth)


def per_device(n, n_tp, *args):
    if n == 8 and n_tp == 4 and len(cut_hidden(args[2].shape[1])) == 3 and args[2].shape[0] % 128 == 0:
        return per_device_fused(n, args)
    return per_device_rings(n, n_tp, *args)


def solution(mesh):
    token = P(("fs", "tp"), None)
    weight = P("fs", "tp")
    return jax.shard_map(
        functools.partial(per_device, mesh.shape["fs"], mesh.shape["tp"]),
        mesh=mesh,
        in_specs=(token, P(), weight, weight, weight, token, token, weight, weight, weight, P()),
        out_specs=(token, token, weight, weight, weight, P()),
        check_vma=False,
    )
```
